32 devices in a mesh: fs: 4 (over y, x), tp: 8 (over z, core).
Axes of the slice: x: 2, y: 2, z: 4, core: 2. Of those that a mesh axis runs over, the one named last changes fastest.
Arguments:
- inputs: bfloat16 [8, 320, 2048], P('tp'), may hold values from -6 to 6
- cotangent: bfloat16 [8, 320, 2048], P('tp'), may hold values from -8 to 8
- gate_weight: bfloat16 [2048, 5632], P('tp', 'fs'), may hold values from -0.125 to 0.125
- up_weight: bfloat16 [2048, 5632], P('tp', 'fs'), may hold values from -0.125 to 0.125
- down_weight: bfloat16 [5632, 2048], P('fs', 'tp'), may hold values from -0.078125 to 0.078125
Outputs:
- input_grad: bfloat16 [8, 320, 2048], P('tp')
- down_grad: float32 [5632, 2048], P('fs', 'tp')
The draws below stay inside these ranges and needn't reach their ends.
All inputs are finite; a program needn't handle non-finite values.
Results may differ from the reference program's by a relative error of at most 0.023.
Values may be sent and summed in bfloat16 or wider, within the bound.
A program may use at most 64 MiB of HBM per device.

```python
import jax
import jax.numpy as jnp
from jax import lax

D = 2048
FF = 5632
TOK_DEV = 320
SPANS = 8
N_FS = 4


def spiked(array, key, source, target, shards_of, factor):
    def block_of(position):
        return (jnp.arange(array.shape[position]) // (array.shape[position] // shards_of)).reshape((-1,) + (1,) * (array.ndim - 1 - position))

    first = jax.random.permutation(key, shards_of)[block_of(target)]
    other_side = (block_of(target) + shards_of // 2) % shards_of
    return jnp.where((block_of(source) == first) | (block_of(source) == other_side), factor * array, array)


def levels(rng, shape, cuts, low, high):
    loudness, own = 1.0, jax.random.fold_in(rng, 6)
    for position, blocks in cuts:
        heights = jnp.exp(jax.random.uniform(jax.random.fold_in(own, position), (blocks,), jnp.float32, low / len(cuts), high / len(cuts)))
        loudness = loudness * jnp.repeat(heights, shape[position] // blocks).reshape([-1 if axis == position else 1 for axis in range(len(shape))])
    return loudness


def centred(stream_key, extent, scale, limit, cuts=(), dtype=jnp.bfloat16):
    values = scale * jax.random.normal(stream_key, extent, jnp.float32)
    if cuts:
        values = values * levels(stream_key, extent, cuts, -0.22, 0.18)
    return jnp.clip(values, -limit, limit).astype(dtype)


def noise_with(own_key, extent, scale, limit, cuts, heavy, kind=jnp.bfloat16):
    array = scale * jax.random.normal(own_key, extent, jnp.float32)
    if cuts:
        array = array * levels(own_key, extent, cuts, -0.22, 0.18)
    return jnp.clip(spiked(array, jax.random.fold_in(own_key, 3), *heavy), -limit, limit).astype(kind)


def setup_inputs(seed: int = 0) -> dict:
    splits = jax.random.split(jax.random.key(seed), 6)
    inputs = centred(splits[0], (SPANS, TOK_DEV, D), 1.0, 6.0, ((0, 8),))
    cotangent = noise_with(splits[1], (SPANS, TOK_DEV, D), 1.0, 8.0, ((0, 8),), (0, 2, 8, 2.0))
    gate_weight = centred(splits[2], (D, FF), D ** -0.5, 0.125, ((0, 8), (1, 4)))
    up_weight = centred(splits[3], (D, FF), D ** -0.5, 0.125, ((0, 8), (1, 4)))
    down_weight = centred(splits[4], (FF, D), FF ** -0.5, 0.078125, ((0, 4), (1, 8)))
    return {"inputs": inputs, "cotangent": cotangent, "gate_weight": gate_weight, "up_weight": up_weight, "down_weight": down_weight}


def reference(inputs, cotangent, gate_weight, up_weight, down_weight):
    rows_in = inputs.reshape(-1, D)
    rows_grad = cotangent.reshape(-1, D)
    gate_pre = jnp.dot(rows_in, gate_weight, preferred_element_type=jnp.float32)
    up_pre = jnp.dot(rows_in, up_weight, preferred_element_type=jnp.float32)
    sig = jax.nn.sigmoid(gate_pre)
    hidden = (gate_pre * sig * up_pre).astype(jnp.bfloat16)
    down_grad = jnp.dot(hidden.T, rows_grad, preferred_element_type=jnp.float32)
    hidden_grad = jnp.dot(rows_grad, down_weight.T, preferred_element_type=jnp.float32)
    gate_grad = (hidden_grad * up_pre * sig * (1.0 + gate_pre * (1.0 - sig))).astype(jnp.bfloat16)
    up_grad = (hidden_grad * gate_pre * sig).astype(jnp.bfloat16)
    width = FF // N_FS
    total_rows = rows_in.shape[0]
    gate_blocks = gate_weight.reshape(D, N_FS, width).transpose(1, 0, 2)
    up_blocks = up_weight.reshape(D, N_FS, width).transpose(1, 0, 2)
    gate_cols = gate_grad.reshape(total_rows, N_FS, width).transpose(1, 0, 2)
    up_cols = up_grad.reshape(total_rows, N_FS, width).transpose(1, 0, 2)

    def add_block(total, pieces):
        g_weight, u_weight, g_cols, u_cols = pieces
        term = jnp.dot(g_cols, g_weight.T, preferred_element_type=jnp.float32)
        term = term + jnp.dot(u_cols, u_weight.T, preferred_element_type=jnp.float32)
        return total + term.astype(jnp.bfloat16).astype(jnp.float32), None

    start_total = jnp.zeros((total_rows, D), jnp.float32)
    total, unused = lax.scan(add_block, start_total, (gate_blocks, up_blocks, gate_cols, up_cols))
    input_grad = total.astype(jnp.bfloat16).reshape(inputs.shape)
    return input_grad, down_grad
```

```python
import functools

import jax
import jax.numpy as jnp
from jax import lax
from jax.experimental import pallas as pl
from jax.experimental.pallas import tpu as pltpu
from jax.sharding import PartitionSpec as P

MESH = pl.DeviceIdType.MESH
BF16 = jnp.bfloat16
F32 = jnp.float32


def contract_hidden(left, right):
    return lax.dot_general(left, right, (((1,), (1,)), ((), ())), preferred_element_type=F32)


def contract_tokens(left, right):
    return lax.dot_general(left, right, (((0,), (0,)), ((), ())), preferred_element_type=F32)


def gathered(inputs, cotangent, gate_weight, up_weight, down_weight):
    rows_in = inputs[0]
    rows_grad = cotangent[0]
    token_count, model_width = rows_in.shape
    gate_full = lax.all_gather(gate_weight, "tp", axis=0, tiled=True)
    up_full = lax.all_gather(up_weight, "tp", axis=0, tiled=True)
    down_tall = lax.all_gather(down_weight.T, "tp", axis=0, tiled=True)
    gate_pre = jnp.dot(rows_in, gate_full, preferred_element_type=F32)
    up_pre = jnp.dot(rows_in, up_full, preferred_element_type=F32)
    sig = jax.nn.sigmoid(gate_pre)
    hidden = (gate_pre * sig * up_pre).astype(BF16)
    hidden_grad = jnp.dot(rows_grad, down_tall, preferred_element_type=F32)
    gate_grad = (hidden_grad * up_pre * sig * (1.0 + gate_pre * (1.0 - sig))).astype(BF16)
    up_grad = (hidden_grad * gate_pre * sig).astype(BF16)
    partial_down = contract_tokens(hidden, rows_grad)
    down_grad = lax.psum_scatter(
        partial_down.astype(BF16), "tp", scatter_dimension=1, tiled=True
    ).astype(F32)
    own_sum = lax.psum_scatter(
        (contract_hidden(gate_grad, gate_full) + contract_hidden(up_grad, up_full)).astype(BF16),
        "fs",
        scatter_dimension=0,
        tiled=True,
    )
    whole_grad = lax.all_gather(own_sum, "fs", axis=0, tiled=True)
    return (whole_grad.reshape(1, token_count, model_width), down_grad)


def kernel(
    n_tp, x_ref, ct_ref, wg_ref, wu_ref, wd_ref, grad_ref, down_ref,
    tok, wts, gate_t, up_t, part, y_in, z_in, acc, gate_g, up_g,
    dn_out, dn_in, dx_out, dx_in, dz_out, dz_in,
    loc_sem, z_ss, y_ss, tok_zs, tok_ys, w_ss, w_rs, x_ss, x_rs, d_ss, d_rs,
    yi_ss, yi_rs, zi_ss, zi_rs, ag_ss, ag_rs, dn_ss, dn_rs, dx_ss, dx_rs, dz_ss, dz_rs,
):
    f, t = lax.axis_index("fs"), lax.axis_index("tp")
    n_z = n_tp // 2
    z, c = t // 2, t % 2
    fy, fx = f // 2, f % 2
    dev_x, dev_y = {"fs": fy * 2 + 1 - fx}, {"fs": (1 - fy) * 2 + fx}
    partner = {"tp": z * 2 + 1 - c}
    half, width = tok.shape[2], tok.shape[3]
    quarter = half // 2
    hid = wts.shape[1] // 2
    cols = width // n_tp
    weights = (gate_t, up_t, wd_ref)

    def plane(p):
        return {"tp": p * 2 + c}

    def rc(src, dst, ss, rs, dev):
        return pltpu.make_async_remote_copy(
            src_ref=src, dst_ref=dst, send_sem=ss, recv_sem=rs, device_id=dev, device_id_type=MESH
        )

    def ds(index, size):
        return pl.ds(pl.multiple_of(index * size, size), size)

    def near(j):
        low = jnp.where(z < n_z // 2, z, n_z - 1 - z)
        step = jnp.where(j % 2 == 1, (j + 1) // 2, -(j // 2))
        p = jnp.where(j <= 2 * low, low + step, j)
        return jnp.where(z < n_z // 2, p, n_z - 1 - p)

    def z_copy(arr, p, d):
        src = tok.at[arr, p, ds(fy, quarter)]
        to = z + 1 if d else z - 1
        return rc(src, src, z_ss.at[arr, p, d], tok_zs.at[arr, p], plane(to))

    def y_copy(arr, p):
        src = tok.at[arr, p, ds(fy, quarter)]
        return rc(src, src, y_ss.at[arr, p], tok_ys.at[arr, p], dev_y)

    def z_tok_wait(arr, p):
        dst = tok.at[arr, p, ds(fy, quarter)]
        rc(dst, dst, y_ss.at[arr, p], tok_zs.at[arr, p], dev_y).wait_recv()

    def y_tok_wait(arr, p):
        dst = tok.at[arr, p, ds(1 - fy, quarter)]
        rc(dst, dst, y_ss.at[arr, p], tok_ys.at[arr, p], dev_y).wait_recv()

    def tok_in(arr, p):
        z_tok_wait(arr, p)

        @pl.when((p < z) & (z < n_z - 1))
        def _():
            z_copy(arr, p, 1).start()

        @pl.when((p > z) & (z > 0))
        def _():
            z_copy(arr, p, 0).start()

        y_copy(arr, p).start()

    def block(i, side, s, core):
        return wts.at[i, ds(side, hid), ds(s * 2 + core, cols)]

    def own_block(i, p):
        return weights[i].at[ds(p, hid)]

    def w_copy(i, to):
        return rc(own_block(i, to), block(i, fx, z, c), w_ss.at[i, to], w_rs.at[i, z], plane(to))

    def x_copy(i, s, src=None):
        dst = block(i, fx, s, c)
        return rc(dst if src is None else src, dst, x_ss.at[i, s], x_rs.at[i, s], dev_x)

    def d_copy(i, other, s, src=None):
        side = 1 - fx if other else fx
        dst = block(i, side, s, c)
        return rc(
            dst if src is None else src, dst, d_ss.at[i, other, s], d_rs.at[i, other, s], partner
        )

    own = [
        pltpu.make_async_copy(x_ref.at[0, ds(fx, half)], tok.at[0, z], loc_sem.at[0]),
        pltpu.make_async_copy(ct_ref.at[0, ds(fx, half)], tok.at[1, z], loc_sem.at[1]),
    ]
    for copy in own:
        copy.start()

    barrier = pltpu.get_barrier_semaphore()
    for dev in (dev_x, dev_y):
        pl.semaphore_signal(barrier, inc=1, device_id=dev, device_id_type=MESH)
    for k in range(1, n_tp):
        pl.semaphore_signal(barrier, inc=1, device_id={"tp": (t + k) % n_tp}, device_id_type=MESH)
    pl.semaphore_wait(barrier, 2 + n_tp - 1)

    for arr in range(2):
        own[arr].wait()
        for d, ok in ((1, z < n_z - 1), (0, z > 0)):
            @pl.when(ok)
            def _(arr=arr, d=d):
                z_copy(arr, z, d).start()

    def w_send(i):
        x_copy(i, z, own_block(i, z)).start()
        d_copy(i, 0, z, own_block(i, z)).start()
        for j in range(1, n_z):
            w_copy(i, near(j)).start()

    w_send(2)
    gate_t[...] = wg_ref[...].T
    w_send(0)
    up_t[...] = wu_ref[...].T
    w_send(1)
    for i in range(3):
        wts[i, ds(fx, hid), ds(t, cols)] = weights[i][ds(z, hid)]
    acc[...] = jnp.zeros_like(acc)

    for arr in range(2):
        for p, ok in ((z + 1, z < n_z - 1), (z - 1, z > 0)):
            @pl.when(ok)
            def _(arr=arr, p=p):
                tok_in(arr, p)

    def w_in(i):
        @pl.loop(1, n_z)
        def _(j):
            s = near(j)
            dst = block(i, fx, s, c)
            rc(dst, dst, w_ss.at[i, s], w_rs.at[i, s], partner).wait_recv()
            x_copy(i, s).start()
            d_copy(i, 0, s).start()

    def x_in(i):
        @pl.loop(0, n_z)
        def _(j):
            s = jnp.where(j == 0, z, near(j))
            dst = block(i, 1 - fx, s, c)
            rc(dst, dst, x_ss.at[i, s], x_rs.at[i, s], partner).wait_recv()
            d_copy(i, 1, s).start()

    w_in(2)
    x_in(2)
    w_in(0)
    x_in(0)
    w_in(1)
    x_in(1)
    for i in range(3):
        for other in range(2):
            side = 1 - fx if other else fx
            for s in range(n_z):
                dst = block(i, side, s, 1 - c)
                rc(dst, dst, d_ss.at[i, other, s], d_rs.at[i, other, s], partner).wait_recv()

    def yi_copy(p):
        return rc(
            part.at[p, ds(1 - fy, quarter)], y_in.at[p], yi_ss.at[p], yi_rs.at[p], dev_y
        )

    def zi_copy(p):
        return rc(part.at[p, ds(fy, quarter)], z_in.at[z], zi_ss.at[p], zi_rs.at[z], plane(p))

    def sweep(p):
        rows, ct = tok[0, p], tok[1, p]

        @pl.loop(0, 2)
        def _(h):
            hs = ds(h, hid)
            gate_pre = contract_hidden(rows, wts[0, hs])
            up_pre = contract_hidden(rows, wts[1, hs])
            hidden_grad = contract_hidden(ct, wts[2, hs])
            sig = jax.nn.sigmoid(gate_pre)
            silu = gate_pre * sig
            hidden = (silu * up_pre).astype(BF16)
            gate_g[h] = (hidden_grad * up_pre * sig * (1.0 + gate_pre * (1.0 - sig))).astype(BF16)
            up_g[h] = (hidden_grad * silu).astype(BF16)
            for n in range(2):
                at = pl.ds(n * (width // 2), width // 2)
                acc[hs, at] += contract_tokens(hidden, ct[:, n * (width // 2) : (n + 1) * (width // 2)])

        @pl.loop(0, 2)
        def _(n):
            at = ds(n, width // 2)
            total = jnp.dot(gate_g[0], wts[0, :hid, at], preferred_element_type=F32)
            total += jnp.dot(up_g[0], wts[1, :hid, at], preferred_element_type=F32)
            total += jnp.dot(gate_g[1], wts[0, hid:, at], preferred_element_type=F32)
            total += jnp.dot(up_g[1], wts[1, hid:, at], preferred_element_type=F32)
            part[p, :, at] = total.astype(BF16)

    def y_add(p):
        dst = y_in.at[p]
        rc(dst, dst, yi_ss.at[p], yi_rs.at[p], dev_y).wait_recv()
        mine = ds(fy, quarter)
        part[p, mine] = (part[p, mine].astype(F32) + y_in[p].astype(F32)).astype(BF16)

        @pl.when(p != z)
        def _():
            zi_copy(p).start()

    def turn(j):
        return jnp.where(j == n_z - 1, z, near(j + 1))

    @pl.loop(0, n_z)
    def _(j):
        p = turn(j)

        @pl.when((p > z + 1) | (p < z - 1))
        def _():
            for arr in range(2):
                tok_in(arr, p)

        @pl.when(p != z)
        def _():
            for arr in range(2):
                y_tok_wait(arr, p)

        sweep(p)
        yi_copy(p).start()

        @pl.when(j > 0)
        def _():
            y_add(turn(j - 1))

    def far(k):
        return jnp.where(k == n_z - 1, z, near(n_z - 1 - k))

    def dn_copy(p):
        return rc(dn_out.at[p], dn_in.at[p], dn_ss.at[p], dn_rs.at[p], partner)

    def dx_copy(p):
        return rc(dx_out.at[p], dx_in.at[p], dx_ss.at[p], dx_rs.at[p], dev_x)

    def dz_copy(p):
        return rc(dz_out.at[p], dz_in.at[z], dz_ss.at[p], dz_rs.at[z], plane(p))

    @pl.loop(0, n_z)
    def _(k):
        p = far(k)
        dn_out[p] = acc[:, ds(p * 2 + 1 - c, cols)].astype(BF16)
        dn_copy(p).start()

    @pl.loop(0, n_z)
    def _(k):
        p = far(k)
        dn_copy(p).wait_recv()
        mine = ds(p * 2 + c, cols)
        other = ds(1 - fx, hid)
        here = ds(fx, hid)
        dx_out[p] = (acc[other, mine] + dn_in[p, other].astype(F32)).astype(BF16)
        dx_copy(p).start()
        acc[here, mine] = acc[here, mine] + dn_in[p, here].astype(F32)

    @pl.loop(0, n_z)
    def _(k):
        p = far(k)
        dx_copy(p).wait_recv()
        total = acc[ds(fx, hid), ds(p * 2 + c, cols)] + dx_in[p].astype(F32)

        @pl.when(p == z)
        def _():
            down_ref[ds(z, hid)] = total

        @pl.when(p != z)
        def _():
            dz_out[p] = total.astype(BF16)
            dz_copy(p).start()

    y_add(z)

    own_rows = ds(fx * 2 + fy, quarter)
    total = part[z, ds(fy, quarter)].astype(F32)
    for j in range(1, n_z):
        s = near(j)
        dst = z_in.at[s]
        rc(dst, dst, zi_ss.at[s], zi_rs.at[s], partner).wait_recv()
        total += z_in[s].astype(F32)
    grad_ref[0, own_rows] = total.astype(BF16)

    def ag_copy(i, rows, dev):
        src = grad_ref.at[0, rows]
        return rc(src, src, ag_ss.at[i], ag_rs.at[i], dev)

    x_rows = ds((1 - fx) * 2 + fy, quarter)
    y_rows = ds(fx * 2 + 1 - fy, quarter)
    d_rows = ds((1 - fx) * 2 + 1 - fy, quarter)
    ag_copy(0, own_rows, dev_x).start()
    ag_copy(1, own_rows, dev_y).start()
    ag_copy(0, x_rows, dev_x).wait_recv()
    ag_copy(2, x_rows, dev_y).start()

    for j in range(1, n_z):
        s = near(j)
        dst = dz_in.at[s]
        rc(dst, dst, dz_ss.at[s], dz_rs.at[s], partner).wait_recv()
        down_ref[ds(s, hid)] = dz_in[s].astype(F32)

    ag_copy(1, y_rows, dev_y).wait_recv()
    ag_copy(2, d_rows, dev_y).wait_recv()

    for arr in range(2):
        for p in range(n_z):
            @pl.when((z < n_z - 1) & (p <= z))
            def _(arr=arr, p=p):
                z_copy(arr, p, 1).wait_send()

            @pl.when((z > 0) & (p >= z))
            def _(arr=arr, p=p):
                z_copy(arr, p, 0).wait_send()

            @pl.when(p != z)
            def _(arr=arr, p=p):
                y_copy(arr, p).wait_send()

    for p in range(n_z):
        for i in range(3):
            x_copy(i, p).wait_send()
            d_copy(i, 0, p).wait_send()
            d_copy(i, 1, p).wait_send()
        yi_copy(p).wait_send()
        dn_copy(p).wait_send()
        dx_copy(p).wait_send()

        @pl.when(p != z)
        def _(p=p):
            for i in range(3):
                w_copy(i, p).wait_send()
            zi_copy(p).wait_send()
            dz_copy(p).wait_send()

    ag_copy(0, own_rows, dev_x).wait_send()
    ag_copy(1, own_rows, dev_y).wait_send()
    ag_copy(2, x_rows, dev_y).wait_send()


def spread(n_tp, inputs, cotangent, gate_weight, up_weight, down_weight):
    _, n_tok, width = inputs.shape
    hid_all = gate_weight.shape[1]
    n_z = n_tp // 2
    hid, cols, half, quarter = hid_all // n_z, width // n_tp, n_tok // 2, n_tok // 4
    dma = pltpu.SemaphoreType.DMA
    vmem = pl.BlockSpec(memory_space=pltpu.VMEM)
    anyspace = pl.BlockSpec(memory_space=pl.ANY)
    return pl.pallas_call(
        functools.partial(kernel, n_tp),
        name="spread_hidden",
        out_shape=(
            jax.ShapeDtypeStruct((1, n_tok, width), BF16),
            jax.ShapeDtypeStruct((hid_all, cols), F32),
        ),
        in_specs=[anyspace, anyspace, vmem, vmem, vmem],
        out_specs=(vmem, vmem),
        scratch_shapes=[
            pltpu.VMEM((2, n_z, half, width), BF16),
            pltpu.VMEM((3, 2 * hid, width), BF16),
            pltpu.VMEM((hid_all, cols), BF16),
            pltpu.VMEM((hid_all, cols), BF16),
            pltpu.VMEM((n_z, half, width), BF16),
            pltpu.VMEM((n_z, quarter, width), BF16),
            pltpu.VMEM((n_z, quarter, width), BF16),
            pltpu.VMEM((2 * hid, width), F32),
            pltpu.VMEM((2, half, hid), BF16),
            pltpu.VMEM((2, half, hid), BF16),
            pltpu.VMEM((n_z, 2 * hid, cols), BF16),
            pltpu.VMEM((n_z, 2 * hid, cols), BF16),
            pltpu.VMEM((n_z, hid, cols), BF16),
            pltpu.VMEM((n_z, hid, cols), BF16),
            pltpu.VMEM((n_z, hid, cols), BF16),
            pltpu.VMEM((n_z, hid, cols), BF16),
            dma((2,)), dma((2, n_z, 2)), dma((2, n_z)), dma((2, n_z)), dma((2, n_z)),
            dma((3, n_z)), dma((3, n_z)), dma((3, n_z)), dma((3, n_z)),
            dma((3, 2, n_z)), dma((3, 2, n_z)),
            dma((n_z,)), dma((n_z,)), dma((n_z,)), dma((n_z,)), dma((3,)), dma((3,)),
            dma((n_z,)), dma((n_z,)), dma((n_z,)), dma((n_z,)), dma((n_z,)), dma((n_z,)),
        ],
        compiler_params=pltpu.CompilerParams(
            collective_id=0, has_side_effects=True, vmem_limit_bytes=66_000_000
        ),
    )(inputs, cotangent, gate_weight, up_weight, down_weight)


def solution(mesh):
    n_fs, n_tp = mesh.shape["fs"], mesh.shape["tp"]

    def per_device(inputs, cotangent, gate_weight, up_weight, down_weight):
        _, n_tok, width = inputs.shape
        hid_all = gate_weight.shape[1]
        n_z = n_tp // 2
        fits = (
            n_fs == 4
            and n_tp % 2 == 0
            and hid_all % (n_z * 16) == 0
            and width % (n_tp * 128) == 0
            and n_tok % 64 == 0
            and (3 * n_tok + 9 * hid_all) * n_z * width + 18 * hid_all * width < 62_000_000 * n_z
        )
        if not fits:
            return gathered(inputs, cotangent, gate_weight, up_weight, down_weight)
        return spread(n_tp, inputs, cotangent, gate_weight, up_weight, down_weight)

    return jax.shard_map(
        per_device,
        mesh=mesh,
        in_specs=(
            P("tp", None, None),
            P("tp", None, None),
            P("tp", "fs"),
            P("tp", "fs"),
            P("fs", "tp"),
        ),
        out_specs=(P("tp", None, None), P("fs", "tp")),
        check_vma=False,
    )
```

```python
import functools

import jax
import jax.numpy as jnp
from jax import lax
from jax.experimental import pallas as pl
from jax.experimental.pallas import tpu as pltpu
from jax.sharding import PartitionSpec as P

MESH = pl.DeviceIdType.MESH
BF16 = jnp.bfloat16
F32 = jnp.float32


def contract_hidden(left, right):
    return lax.dot_general(left, right, (((1,), (1,)), ((), ())), preferred_element_type=F32)


def contract_tokens(left, right):
    return lax.dot_general(left, right, (((0,), (0,)), ((), ())), preferred_element_type=F32)


def gathered(inputs, cotangent, gate_weight, up_weight, down_weight):
    rows_in = inputs[0]
    rows_grad = cotangent[0]
    token_count, model_width = rows_in.shape
    gate_full = lax.all_gather(gate_weight, "tp", axis=0, tiled=True)
    up_full = lax.all_gather(up_weight, "tp", axis=0, tiled=True)
    down_tall = lax.all_gather(down_weight.T, "tp", axis=0, tiled=True)
    gate_pre = jnp.dot(rows_in, gate_full, preferred_element_type=F32)
    up_pre = jnp.dot(rows_in, up_full, preferred_element_type=F32)
    sig = jax.nn.sigmoid(gate_pre)
    hidden = (gate_pre * sig * up_pre).astype(BF16)
    hidden_grad = jnp.dot(rows_grad, down_tall, preferred_element_type=F32)
    gate_grad = (hidden_grad * up_pre * sig * (1.0 + gate_pre * (1.0 - sig))).astype(BF16)
    up_grad = (hidden_grad * gate_pre * sig).astype(BF16)
    partial_down = contract_tokens(hidden, rows_grad)
    down_grad = lax.psum_scatter(
        partial_down.astype(BF16), "tp", scatter_dimension=1, tiled=True
    ).astype(F32)
    own_sum = lax.psum_scatter(
        (contract_hidden(gate_grad, gate_full) + contract_hidden(up_grad, up_full)).astype(BF16),
        "fs",
        scatter_dimension=0,
        tiled=True,
    )
    whole_grad = lax.all_gather(own_sum, "fs", axis=0, tiled=True)
    return (whole_grad.reshape(1, token_count, model_width), down_grad)


def kernel(
    n_tp, x_ref, ct_ref, wg_ref, wu_ref, wd_ref, grad_ref, down_ref,
    tok, wts, gate_t, up_t, part, y_in, z_in, acc, pre, gate_g, up_g, hidden_b,
    dn_out, dn_in, dx_out, dx_in, dz_out, dz_in, fwd,
    loc_sem, z_ss, y_ss, tok_zs, tok_ys, w_ss, w_rs, x_ss, x_rs, d_ss, d_rs,
    yi_ss, yi_rs, zi_ss, zi_rs, ag_ss, ag_rs, dn_ss, dn_rs, dx_ss, dx_rs, dz_ss, dz_rs,
):
    f, t = lax.axis_index("fs"), lax.axis_index("tp")
    n_z = n_tp // 2
    z, c = t // 2, t % 2
    fy, fx = f // 2, f % 2
    dev_x, dev_y = {"fs": fy * 2 + 1 - fx}, {"fs": (1 - fy) * 2 + fx}
    partner = {"tp": z * 2 + 1 - c}
    half, width = tok.shape[1] // n_z, tok.shape[2]
    quarter = half // 2
    hid = wts.shape[2] // 2
    cols = width // n_tp
    weights = (gate_t, up_t, wd_ref)

    def plane(p):
        return {"tp": p * 2 + c}

    def rc(src, dst, ss, rs, dev):
        return pltpu.make_async_remote_copy(
            src_ref=src, dst_ref=dst, send_sem=ss, recv_sem=rs, device_id=dev, device_id_type=MESH
        )

    def ds(index, size):
        return pl.ds(pl.multiple_of(index * size, size), size)

    def near(j):
        low = jnp.where(z < n_z // 2, z, n_z - 1 - z)
        step = jnp.where(j % 2 == 1, (j + 1) // 2, -(j // 2))
        p = jnp.where(j <= 2 * low, low + step, j)
        return jnp.where(z < n_z // 2, p, n_z - 1 - p)

    def tok_rows(arr, p, side):
        start = pl.multiple_of(p * half + side * quarter, quarter)
        return tok.at[arr, pl.ds(start, quarter)]

    def z_copy(arr, p, d):
        src = tok_rows(arr, p, fy)
        to = z + 1 if d else z - 1
        return rc(src, src, z_ss.at[arr, p, d], tok_zs.at[arr, p], plane(to))

    def y_copy(arr, p):
        src = tok_rows(arr, p, fy)
        return rc(src, src, y_ss.at[arr, p], tok_ys.at[arr, p], dev_y)

    def z_tok_wait(arr, p):
        dst = tok_rows(arr, p, fy)
        rc(dst, dst, y_ss.at[arr, p], tok_zs.at[arr, p], dev_y).wait_recv()

    def y_tok_wait(arr, p):
        dst = tok_rows(arr, p, 1 - fy)
        rc(dst, dst, y_ss.at[arr, p], tok_ys.at[arr, p], dev_y).wait_recv()

    def tok_in(arr, p):
        z_tok_wait(arr, p)

        @pl.when((p < z) & (z < n_z - 1))
        def _():
            z_copy(arr, p, 1).start()

        @pl.when((p > z) & (z > 0))
        def _():
            z_copy(arr, p, 0).start()

        y_copy(arr, p).start()

    def block(i, side, s, core):
        return wts.at[i, s * 2 + core, ds(side, hid)]

    def own_block(i, p):
        return weights[i].at[ds(p, hid)]

    def w_wait(i, s, to):
        dst = fwd.at[i, s, to]
        rc(dst, dst, w_ss.at[i, s, to], w_rs.at[i, s, to], partner).wait_recv()

    def w_hop(i, s, to, src):
        via = jnp.where(to > z, z + 1, z - 1)
        sems = (w_ss.at[i, s, to], w_rs.at[i, s, to], plane(via))

        @pl.when(via == to)
        def _():
            rc(src, block(i, fx, s, c), *sems).start()

        @pl.when(via != to)
        def _():
            rc(src, fwd.at[i, s, to], *sems).start()

    def x_copy(i, s, src=None):
        dst = block(i, fx, s, c)
        return rc(dst if src is None else src, dst, x_ss.at[i, s], x_rs.at[i, s], dev_x)

    def d_copy(i, other, s, src=None):
        side = 1 - fx if other else fx
        dst = block(i, side, s, c)
        return rc(
            dst if src is None else src, dst, d_ss.at[i, other, s], d_rs.at[i, other, s], partner
        )

    own = [
        pltpu.make_async_copy(x_ref.at[0, ds(fx, half)], tok.at[0, ds(z, half)], loc_sem.at[0]),
        pltpu.make_async_copy(ct_ref.at[0, ds(fx, half)], tok.at[1, ds(z, half)], loc_sem.at[1]),
    ]
    for copy in own:
        copy.start()

    barrier = pltpu.get_barrier_semaphore()
    for dev in (dev_x, dev_y):
        pl.semaphore_signal(barrier, inc=1, device_id=dev, device_id_type=MESH)
    for k in range(1, n_tp):
        pl.semaphore_signal(barrier, inc=1, device_id={"tp": (t + k) % n_tp}, device_id_type=MESH)
    pl.semaphore_wait(barrier, 2 + n_tp - 1)

    for arr in range(2):
        own[arr].wait()
        for d, ok in ((1, z < n_z - 1), (0, z > 0)):
            @pl.when(ok)
            def _(arr=arr, d=d):
                z_copy(arr, z, d).start()

    order_i = (2, 0, 1)

    def w_own(i):
        x_copy(i, z, own_block(i, z)).start()
        d_copy(i, 0, z, own_block(i, z)).start()
        for e in range(1, n_z):
            for to, ok in ((z + e, z + e < n_z), (z - e, z >= e)):
                if e == 1:
                    @pl.when(ok)
                    def _(to=to):
                        w_hop(i, z, to, own_block(i, to))

    w_own(2)
    gate_t[...] = wg_ref[...].T
    w_own(0)
    up_t[...] = wu_ref[...].T
    w_own(1)
    for e in range(2, n_z):
        for i in order_i:
            for to, ok in ((z + e, z + e < n_z), (z - e, z >= e)):
                @pl.when(ok)
                def _(i=i, to=to):
                    w_hop(i, z, to, own_block(i, to))
    for i in range(3):
        wts[i, t, ds(fx, hid)] = weights[i][ds(z, hid)]
    acc[...] = jnp.zeros_like(acc)
    pre[...] = jnp.zeros_like(pre)

    def sides(g):
        return ((z - g, z >= g, 1), (z + g, z + g < n_z, -1))

    def w_in(i, s):
        w_wait(i, s, z)
        x_copy(i, s).start()
        d_copy(i, 0, s).start()

    last = jnp.where(z < n_z // 2, n_z - 1, 0)

    def x_in(i, s):
        dst = block(i, 1 - fx, s, c)
        rc(dst, dst, x_ss.at[i, s], x_rs.at[i, s], partner).wait_recv()
        d_copy(i, 1, s).start()

    def unit(p, s):
        rows = ds(p, half)
        for i in range(3):
            total = pre[i, rows]
            for k in range(2):
                at = ds(s * 2 + k, cols)
                total += contract_hidden(tok[1 if i == 2 else 0, rows, at], wts[i, s * 2 + k])
            pre[i, rows] = total

    def arrived(i, s):
        for other in range(2):
            side = 1 - fx if other else fx
            dst = block(i, side, s, 1 - c)
            rc(dst, dst, d_ss.at[i, other, s], d_rs.at[i, other, s], partner).wait_recv()

    def finish(g):
        for k, (s, ok, _) in enumerate(sides(g)):
            @pl.when(ok & (s != last))
            def _(k=k, s=s):
                for i in order_i:
                    x_in(i, s)
                for arr in range(2):
                    y_tok_wait(arr, s)
                for i in order_i:
                    arrived(i, s)
                unit(s, s)

                @pl.loop(0, n_z)
                def _(r):
                    dist = jnp.where(r > z, r - z, z - r)
                    known = dist < g
                    if k == 1:
                        known = known | (r == z - g)

                    @pl.when(known)
                    def _():
                        unit(s, r)
                        unit(r, s)

    for g in range(1, n_z):
        for arr in range(2):
            for s, ok, _ in sides(g):
                @pl.when(ok)
                def _(arr=arr, s=s):
                    tok_in(arr, s)
        if g == 1:
            for i in order_i:
                x_in(i, z)
                arrived(i, z)
            unit(z, z)
        else:
            finish(g - 1)
        for i in order_i:
            for s, ok, _ in sides(g):
                @pl.when(ok)
                def _(i=i, s=s):
                    w_in(i, s)
        for e in range(1, n_z - g):
            for i in order_i:
                for s, ok, step in sides(g):
                    to = z + step * e

                    @pl.when(ok & (to >= 0) & (to < n_z))
                    def _(i=i, s=s, to=to):
                        w_wait(i, s, to)
                        w_hop(i, s, to, fwd.at[i, s, to])
    for arr in range(2):
        y_tok_wait(arr, last)

    @pl.loop(0, n_z)
    def _(r):
        @pl.when(r != last)
        def _():
            unit(last, r)

    def whole(i):
        arrived(i, last)

        @pl.loop(0, n_z // 2)
        def _(m):
            rows = ds(m, 2 * half)
            total = pre[i, rows]
            for k in range(2):
                at = ds(last * 2 + k, cols)
                total += contract_hidden(tok[1 if i == 2 else 0, rows, at], wts[i, last * 2 + k])
            pre[i, rows] = total

    x_in(2, last)
    x_in(0, last)
    whole(2)
    x_in(1, last)
    whole(0)
    whole(1)

    def yi_copy(p):
        return rc(
            part.at[p, ds(1 - fy, quarter)], y_in.at[p], yi_ss.at[p], yi_rs.at[p], dev_y
        )

    top = z // (n_z // 2)

    def zi_copy(p):
        away = p // (n_z // 2) != top
        step = jnp.where(p > z, z + 1, z - 1)
        to = jnp.where(away & (step // (n_z // 2) != top), p, step)
        slot = jnp.where(to != p, p, jnp.where(away, n_z + 1, jnp.where(p < z, n_z, p)))
        return rc(part.at[p, ds(fy, quarter)], z_in.at[slot], zi_ss.at[p], zi_rs.at[slot], plane(to))

    def zi_wait(slot):
        dst = z_in.at[slot]
        rc(dst, dst, zi_ss.at[0], zi_rs.at[slot], partner).wait_recv()

    def sweep(p):
        @pl.loop(0, half // 32)
        def _(r):
            at = ds(p * (half // 32) + r, 32)
            to = ds(r, 32)
            gate_pre, up_pre, hidden_grad = pre[0, at], pre[1, at], pre[2, at]
            sig = jax.nn.sigmoid(gate_pre)
            silu = gate_pre * sig
            hidden_b[to] = (silu * up_pre).astype(BF16)
            gate_g[to] = (hidden_grad * up_pre * sig * (1.0 + gate_pre * (1.0 - sig))).astype(BF16)
            up_g[to] = (hidden_grad * silu).astype(BF16)

        @pl.loop(0, n_tp)
        def _(n):
            part[p, :, ds(n, cols)] = (
                jnp.dot(gate_g[...], wts[0, n], preferred_element_type=F32)
                + jnp.dot(up_g[...], wts[1, n], preferred_element_type=F32)
            ).astype(BF16)

        yi_copy(p).start()

        @pl.loop(0, 2)
        def _(n):
            at = ds(n, width // 2)
            acc[:, at] += contract_tokens(hidden_b[...], tok[1, ds(p, half), at])

    def y_add(p):
        dst = y_in.at[p]
        rc(dst, dst, yi_ss.at[p], yi_rs.at[p], dev_y).wait_recv()

        @pl.when(p != z)
        def _():
            mine = ds(fy, quarter)
            part[p, mine] = (part[p, mine].astype(F32) + y_in[p].astype(F32)).astype(BF16)

            up = jnp.where(p > z, z - 1, z + 1)

            @pl.when((up >= 0) & (up < n_z) & (up // (n_z // 2) == top))
            def _():
                zi_wait(p)
                part[p, mine] = (part[p, mine].astype(F32) + z_in[p].astype(F32)).astype(BF16)

            zi_copy(p).start()

    def far(k):
        return jnp.where(k == n_z - 1, z, near(n_z - 1 - k))

    @pl.loop(0, n_z)
    def _(j):
        sweep(far(j))

        @pl.when(j == 2)
        def _():
            y_add(far(0))

    def dn_copy(p):
        return rc(dn_out.at[p], dn_in.at[p], dn_ss.at[p], dn_rs.at[p], partner)

    def dx_copy(p):
        return rc(dx_out.at[p], dx_in.at[p], dx_ss.at[p], dx_rs.at[p], dev_x)

    def dz_copy(p):
        return rc(dz_out.at[p], dz_in.at[z], dz_ss.at[p], dz_rs.at[z], plane(p))

    @pl.loop(0, n_z)
    def _(k):
        p = far(k)
        dn_out[p] = acc[:, ds(p * 2 + 1 - c, cols)].astype(BF16)
        dn_copy(p).start()

    @pl.loop(0, n_z)
    def _(k):
        p = far(k)
        dn_copy(p).wait_recv()
        mine = ds(p * 2 + c, cols)
        other = ds(1 - fx, hid)
        here = ds(fx, hid)
        dx_out[p] = (acc[other, mine] + dn_in[p, other].astype(F32)).astype(BF16)
        dx_copy(p).start()
        acc[here, mine] = acc[here, mine] + dn_in[p, here].astype(F32)

    def dx_add(p):
        dx_copy(p).wait_recv()
        total = acc[ds(fx, hid), ds(p * 2 + c, cols)] + dx_in[p].astype(F32)

        @pl.when(p == z)
        def _():
            down_ref[ds(z, hid)] = total

        @pl.when(p != z)
        def _():
            dz_out[p] = total.astype(BF16)
            dz_copy(p).start()

    @pl.loop(1, n_z)
    def _(k):
        dx_add(far(k - 1))
        y_add(far(k))

    own_rows = ds(fx * 2 + fy, quarter)
    def gain(slot):
        zi_wait(slot)
        y_in[z] = (y_in[z].astype(F32) + z_in[slot].astype(F32)).astype(BF16)

    @pl.when((z > 0) & ((z - 1) // (n_z // 2) == top))
    def _():
        gain(z)

    @pl.when((z < n_z - 1) & ((z + 1) // (n_z // 2) == top))
    def _():
        gain(n_z)

    gain(n_z + 1)
    total = part[z, ds(fy, quarter)].astype(F32) + y_in[z].astype(F32)
    grad_ref[0, own_rows] = total.astype(BF16)
    span = width // 4

    def ag_copy(i, n, rows, dev):
        src = grad_ref.at[0, rows, pl.ds(n * span, span)]
        return rc(src, src, ag_ss.at[i, n], ag_rs.at[i, n], dev)

    x_rows = ds((1 - fx) * 2 + fy, quarter)
    y_rows = ds(fx * 2 + 1 - fy, quarter)
    d_rows = ds((1 - fx) * 2 + 1 - fy, quarter)
    for n in range(4):
        ag_copy(1, n, own_rows, dev_y).start()
        ag_copy(0, n, own_rows, dev_x).start()
    dx_add(z)
    for n in range(4):
        ag_copy(1, n, y_rows, dev_y).wait_recv()
        ag_copy(2, n, y_rows, dev_x).start()

    for j in range(1, n_z):
        s = near(j)
        dst = dz_in.at[s]
        rc(dst, dst, dz_ss.at[s], dz_rs.at[s], partner).wait_recv()
        down_ref[ds(s, hid)] = dz_in[s].astype(F32)

    for n in range(4):
        ag_copy(0, n, x_rows, dev_x).wait_recv()
        ag_copy(2, n, d_rows, dev_x).wait_recv()

    for arr in range(2):
        for p in range(n_z):
            @pl.when((z < n_z - 1) & (p <= z))
            def _(arr=arr, p=p):
                z_copy(arr, p, 1).wait_send()

            @pl.when((z > 0) & (p >= z))
            def _(arr=arr, p=p):
                z_copy(arr, p, 0).wait_send()

            @pl.when(p != z)
            def _(arr=arr, p=p):
                y_copy(arr, p).wait_send()

    for p in range(n_z):
        for i in range(3):
            x_copy(i, p).wait_send()
            d_copy(i, 0, p).wait_send()
            d_copy(i, 1, p).wait_send()
        yi_copy(p).wait_send()
        dn_copy(p).wait_send()
        dx_copy(p).wait_send()

        @pl.when(p != z)
        def _(p=p):
            zi_copy(p).wait_send()
            dz_copy(p).wait_send()

    for s in range(n_z):
        for to in range(n_z):
            if s == to:
                continue

            @pl.when((z >= s) & (z < to) if s < to else (z <= s) & (z > to))
            def _(s=s, to=to):
                for i in range(3):
                    src = fwd.at[i, s, to]
                    rc(src, src, w_ss.at[i, s, to], w_rs.at[i, s, to], partner).wait_send()

    for n in range(4):
        ag_copy(0, n, own_rows, dev_x).wait_send()
        ag_copy(1, n, own_rows, dev_y).wait_send()
        ag_copy(2, n, y_rows, dev_x).wait_send()


def spread(n_tp, inputs, cotangent, gate_weight, up_weight, down_weight):
    _, n_tok, width = inputs.shape
    hid_all = gate_weight.shape[1]
    n_z = n_tp // 2
    hid, cols, half, quarter = hid_all // n_z, width // n_tp, n_tok // 2, n_tok // 4
    dma = pltpu.SemaphoreType.DMA
    vmem = pl.BlockSpec(memory_space=pltpu.VMEM)
    anyspace = pl.BlockSpec(memory_space=pl.ANY)
    return pl.pallas_call(
        functools.partial(kernel, n_tp),
        name="spread_hidden",
        out_shape=(
            jax.ShapeDtypeStruct((1, n_tok, width), BF16),
            jax.ShapeDtypeStruct((hid_all, cols), F32),
        ),
        in_specs=[anyspace, anyspace, vmem, vmem, vmem],
        out_specs=(vmem, vmem),
        scratch_shapes=[
            pltpu.VMEM((2, n_z * half, width), BF16),
            pltpu.VMEM((3, n_tp, 2 * hid, cols), BF16),
            pltpu.VMEM((hid_all, cols), BF16),
            pltpu.VMEM((hid_all, cols), BF16),
            pltpu.VMEM((n_z, half, width), BF16),
            pltpu.VMEM((n_z, quarter, width), BF16),
            pltpu.VMEM((n_z + 2, quarter, width), BF16),
            pltpu.VMEM((2 * hid, width), F32),
            pltpu.VMEM((3, n_z * half, 2 * hid), F32),
            pltpu.VMEM((half, 2 * hid), BF16),
            pltpu.VMEM((half, 2 * hid), BF16),
            pltpu.VMEM((half, 2 * hid), BF16),
            pltpu.VMEM((n_z, 2 * hid, cols), BF16),
            pltpu.VMEM((n_z, 2 * hid, cols), BF16),
            pltpu.VMEM((n_z, hid, cols), BF16),
            pltpu.VMEM((n_z, hid, cols), BF16),
            pltpu.VMEM((n_z, hid, cols), BF16),
            pltpu.VMEM((n_z, hid, cols), BF16),
            pltpu.VMEM((3, n_z, n_z, hid, cols), BF16),
            dma((2,)), dma((2, n_z, 2)), dma((2, n_z)), dma((2, n_z)), dma((2, n_z)),
            dma((3, n_z, n_z)), dma((3, n_z, n_z)), dma((3, n_z)), dma((3, n_z)),
            dma((3, 2, n_z)), dma((3, 2, n_z)),
            dma((n_z,)), dma((n_z,)), dma((n_z,)), dma((n_z + 2,)), dma((3, 4)), dma((3, 4)),
            dma((n_z,)), dma((n_z,)), dma((n_z,)), dma((n_z,)), dma((n_z,)), dma((n_z,)),
        ],
        compiler_params=pltpu.CompilerParams(
            collective_id=0, has_side_effects=True, vmem_limit_bytes=66_000_000
        ),
    )(inputs, cotangent, gate_weight, up_weight, down_weight)


def solution(mesh):
    n_fs, n_tp = mesh.shape["fs"], mesh.shape["tp"]

    def per_device(inputs, cotangent, gate_weight, up_weight, down_weight):
        _, n_tok, width = inputs.shape
        hid_all = gate_weight.shape[1]
        n_z = n_tp // 2
        fits = (
            n_fs == 4
            and n_tp % 2 == 0
            and hid_all % (n_z * 16) == 0
            and width % (n_tp * 128) == 0
            and n_tok % 64 == 0
            and (3 * n_tok + 9 * hid_all) * n_z * width + 18 * hid_all * width < 62_000_000 * n_z
        )
        if not fits:
            return gathered(inputs, cotangent, gate_weight, up_weight, down_weight)
        return spread(n_tp, inputs, cotangent, gate_weight, up_weight, down_weight)

    return jax.shard_map(
        per_device,
        mesh=mesh,
        in_specs=(
            P("tp", None, None),
            P("tp", None, None),
            P("tp", "fs"),
            P("tp", "fs"),
            P("fs", "tp"),
        ),
        out_specs=(P("tp", None, None), P("fs", "tp")),
        check_vma=False,
    )
```

```python
import functools

import jax
import jax.numpy as jnp
from jax import lax
from jax.experimental import pallas as pl
from jax.experimental.pallas import tpu as pltpu
from jax.sharding import PartitionSpec as P

MESH = pl.DeviceIdType.MESH
BF16 = jnp.bfloat16
F32 = jnp.float32


def contract_hidden(left, right):
    return lax.dot_general(left, right, (((1,), (1,)), ((), ())), preferred_element_type=F32)


def contract_tokens(left, right):
    return lax.dot_general(left, right, (((0,), (0,)), ((), ())), preferred_element_type=F32)


def gathered(inputs, cotangent, gate_weight, up_weight, down_weight):
    rows_in = inputs[0]
    rows_grad = cotangent[0]
    token_count, model_width = rows_in.shape
    gate_full = lax.all_gather(gate_weight, "tp", axis=0, tiled=True)
    up_full = lax.all_gather(up_weight, "tp", axis=0, tiled=True)
    down_tall = lax.all_gather(down_weight.T, "tp", axis=0, tiled=True)
    gate_pre = jnp.dot(rows_in, gate_full, preferred_element_type=F32)
    up_pre = jnp.dot(rows_in, up_full, preferred_element_type=F32)
    sig = jax.nn.sigmoid(gate_pre)
    hidden = (gate_pre * sig * up_pre).astype(BF16)
    hidden_grad = jnp.dot(rows_grad, down_tall, preferred_element_type=F32)
    gate_grad = (hidden_grad * up_pre * sig * (1.0 + gate_pre * (1.0 - sig))).astype(BF16)
    up_grad = (hidden_grad * gate_pre * sig).astype(BF16)
    partial_down = contract_tokens(hidden, rows_grad)
    down_grad = lax.psum_scatter(
        partial_down.astype(BF16), "tp", scatter_dimension=1, tiled=True
    ).astype(F32)
    own_sum = lax.psum_scatter(
        (contract_hidden(gate_grad, gate_full) + contract_hidden(up_grad, up_full)).astype(BF16),
        "fs",
        scatter_dimension=0,
        tiled=True,
    )
    whole_grad = lax.all_gather(own_sum, "fs", axis=0, tiled=True)
    return (whole_grad.reshape(1, token_count, model_width), down_grad)


def kernel(
    n_tp, x_ref, ct_ref, wg_ref, wu_ref, wd_ref, grad_ref, down_ref,
    tok, wts, gate_t, up_t, part, y_in, z_in, acc, pre, gate_g, up_g, hidden_b, total,
    dn_out, dn_in, dx_out, dx_in, dz_out, dz_in, fwd,
    loc_sem, z_ss, y_ss, tok_zs, tok_ys, w_ss, w_rs, x_ss, x_rs, d_ss, d_rs,
    yi_ss, yi_rs, zi_ss, zi_rs, ag_ss, ag_rs, dn_ss, dn_rs, dx_ss, dx_rs, dz_ss, dz_rs,
):
    f, t = lax.axis_index("fs"), lax.axis_index("tp")
    n_z = n_tp // 2
    z, c = t // 2, t % 2
    fy, fx = f // 2, f % 2
    dev_x, dev_y = {"fs": fy * 2 + 1 - fx}, {"fs": (1 - fy) * 2 + fx}
    partner = {"tp": z * 2 + 1 - c}
    half, width = tok.shape[1] // n_z, tok.shape[2]
    quarter = half // 2
    hid = wts.shape[2] // 2
    cols = width // n_tp
    weights = (gate_t, up_t, wd_ref)

    def plane(p):
        return {"tp": p * 2 + c}

    def rc(src, dst, ss, rs, dev):
        return pltpu.make_async_remote_copy(
            src_ref=src, dst_ref=dst, send_sem=ss, recv_sem=rs, device_id=dev, device_id_type=MESH
        )

    def ds(index, size):
        return pl.ds(pl.multiple_of(index * size, size), size)

    def near(j):
        low = jnp.where(z < n_z // 2, z, n_z - 1 - z)
        step = jnp.where(j % 2 == 1, (j + 1) // 2, -(j // 2))
        p = jnp.where(j <= 2 * low, low + step, j)
        return jnp.where(z < n_z // 2, p, n_z - 1 - p)

    def tok_rows(arr, p, side):
        start = pl.multiple_of(p * half + side * quarter, quarter)
        return tok.at[arr, pl.ds(start, quarter)]

    def z_copy(arr, p, d):
        src = tok_rows(arr, p, fy)
        to = z + 1 if d else z - 1
        return rc(src, src, z_ss.at[arr, p, d], tok_zs.at[arr, p], plane(to))

    def y_copy(arr, p):
        src = tok_rows(arr, p, fy)
        return rc(src, src, y_ss.at[arr, p], tok_ys.at[arr, p], dev_y)

    def z_tok_wait(arr, p):
        dst = tok_rows(arr, p, fy)
        rc(dst, dst, y_ss.at[arr, p], tok_zs.at[arr, p], dev_y).wait_recv()

    def y_tok_wait(arr, p):
        dst = tok_rows(arr, p, 1 - fy)
        rc(dst, dst, y_ss.at[arr, p], tok_ys.at[arr, p], dev_y).wait_recv()

    def tok_in(arr, p):
        z_tok_wait(arr, p)

        @pl.when((p < z) & (z < n_z - 1))
        def _():
            z_copy(arr, p, 1).start()

        @pl.when((p > z) & (z > 0))
        def _():
            z_copy(arr, p, 0).start()

        y_copy(arr, p).start()

    def block(i, side, s, core):
        return wts.at[i, s * 2 + core, ds(side, hid)]

    def own_block(i, p):
        return weights[i].at[ds(p, hid)]

    def w_wait(i, s, to):
        dst = fwd.at[i, s, to]
        rc(dst, dst, w_ss.at[i, s, to], w_rs.at[i, s, to], partner).wait_recv()

    def w_hop(i, s, to, src):
        via = jnp.where(to > z, z + 1, z - 1)
        sems = (w_ss.at[i, s, to], w_rs.at[i, s, to], plane(via))

        @pl.when(via == to)
        def _():
            rc(src, block(i, fx, s, c), *sems).start()

        @pl.when(via != to)
        def _():
            rc(src, fwd.at[i, s, to], *sems).start()

    def x_copy(i, s, src=None):
        dst = block(i, fx, s, c)
        return rc(dst if src is None else src, dst, x_ss.at[i, s], x_rs.at[i, s], dev_x)

    def d_copy(i, other, s, src=None):
        side = 1 - fx if other else fx
        dst = block(i, side, s, c)
        return rc(
            dst if src is None else src, dst, d_ss.at[i, other, s], d_rs.at[i, other, s], partner
        )

    own = [
        pltpu.make_async_copy(x_ref.at[0, ds(fx, half)], tok.at[0, ds(z, half)], loc_sem.at[0]),
        pltpu.make_async_copy(ct_ref.at[0, ds(fx, half)], tok.at[1, ds(z, half)], loc_sem.at[1]),
    ]
    for copy in own:
        copy.start()

    barrier = pltpu.get_barrier_semaphore()
    for dev in (dev_x, dev_y):
        pl.semaphore_signal(barrier, inc=1, device_id=dev, device_id_type=MESH)
    for k in range(1, n_tp):
        pl.semaphore_signal(barrier, inc=1, device_id={"tp": (t + k) % n_tp}, device_id_type=MESH)
    pl.semaphore_wait(barrier, 2 + n_tp - 1)

    for arr in range(2):
        own[arr].wait()
        for d, ok in ((1, z < n_z - 1), (0, z > 0)):
            @pl.when(ok)
            def _(arr=arr, d=d):
                z_copy(arr, z, d).start()

    order_i = (2, 0, 1)

    def w_own(i):
        x_copy(i, z, own_block(i, z)).start()
        d_copy(i, 0, z, own_block(i, z)).start()
        for e in range(1, n_z):
            for to, ok in ((z + e, z + e < n_z), (z - e, z >= e)):
                if e == 1:
                    @pl.when(ok)
                    def _(to=to):
                        w_hop(i, z, to, own_block(i, to))

    w_own(2)
    gate_t[...] = wg_ref[...].T
    w_own(0)
    up_t[...] = wu_ref[...].T
    w_own(1)
    for e in range(2, n_z):
        for i in order_i:
            for to, ok in ((z + e, z + e < n_z), (z - e, z >= e)):
                @pl.when(ok)
                def _(i=i, to=to):
                    w_hop(i, z, to, own_block(i, to))
    for i in range(3):
        wts[i, t, ds(fx, hid)] = weights[i][ds(z, hid)]
    acc[...] = jnp.zeros_like(acc)
    pre[...] = jnp.zeros_like(pre)

    def sides(g):
        return ((z - g, z >= g, 1), (z + g, z + g < n_z, -1))

    def w_in(i, s):
        w_wait(i, s, z)
        x_copy(i, s).start()
        d_copy(i, 0, s).start()

    last = jnp.where(z < n_z // 2, n_z - 1, 0)

    def x_in(i, s):
        dst = block(i, 1 - fx, s, c)
        rc(dst, dst, x_ss.at[i, s], x_rs.at[i, s], partner).wait_recv()
        d_copy(i, 1, s).start()

    def unit(p, s):
        rows = ds(p, half)
        for i in range(3):
            total = pre[i, rows]
            for k in range(2):
                at = ds(s * 2 + k, cols)
                total += contract_hidden(tok[1 if i == 2 else 0, rows, at], wts[i, s * 2 + k])
            pre[i, rows] = total

    def arrived(i, s):
        for other in range(2):
            side = 1 - fx if other else fx
            dst = block(i, side, s, 1 - c)
            rc(dst, dst, d_ss.at[i, other, s], d_rs.at[i, other, s], partner).wait_recv()

    def finish(g):
        for k, (s, ok, _) in enumerate(sides(g)):
            @pl.when(ok & (s != last))
            def _(k=k, s=s):
                for i in order_i:
                    x_in(i, s)
                for arr in range(2):
                    y_tok_wait(arr, s)
                for i in order_i:
                    arrived(i, s)
                unit(s, s)

                @pl.loop(0, n_z)
                def _(r):
                    dist = jnp.where(r > z, r - z, z - r)
                    known = dist < g
                    if k == 1:
                        known = known | (r == z - g)

                    @pl.when(known)
                    def _():
                        unit(s, r)
                        unit(r, s)

    for g in range(1, n_z):
        for arr in range(2):
            for s, ok, _ in sides(g):
                @pl.when(ok)
                def _(arr=arr, s=s):
                    tok_in(arr, s)
        if g == 1:
            for i in order_i:
                x_in(i, z)
                arrived(i, z)
            unit(z, z)
        else:
            finish(g - 1)
        for i in order_i:
            for s, ok, _ in sides(g):
                @pl.when(ok)
                def _(i=i, s=s):
                    w_in(i, s)
        for e in range(1, n_z - g):
            for i in order_i:
                for s, ok, step in sides(g):
                    to = z + step * e

                    @pl.when(ok & (to >= 0) & (to < n_z))
                    def _(i=i, s=s, to=to):
                        w_wait(i, s, to)
                        w_hop(i, s, to, fwd.at[i, s, to])
    for arr in range(2):
        y_tok_wait(arr, last)

    @pl.loop(0, n_z)
    def _(r):
        @pl.when(r != last)
        def _():
            unit(last, r)

    def whole(i):
        arrived(i, last)

        @pl.loop(0, n_z // 2)
        def _(m):
            rows = ds(m, 2 * half)
            total = pre[i, rows]
            for k in range(2):
                at = ds(last * 2 + k, cols)
                total += contract_hidden(tok[1 if i == 2 else 0, rows, at], wts[i, last * 2 + k])
            pre[i, rows] = total

    x_in(2, last)
    x_in(0, last)
    whole(2)
    x_in(1, last)
    whole(0)
    whole(1)

    n_cut = 4
    cut = width // n_cut

    def yi_copy(p, n):
        at = ds(n, cut)
        return rc(
            part.at[p, ds(1 - fy, quarter), at], y_in.at[p, :, at],
            yi_ss.at[p, n], yi_rs.at[p, n], dev_y,
        )

    top = z // (n_z // 2)

    def zi_copy(p, n):
        away = p // (n_z // 2) != top
        step = jnp.where(p > z, z + 1, z - 1)
        to = jnp.where(away & (step // (n_z // 2) != top), p, step)
        slot = jnp.where(to != p, p, jnp.where(away, n_z + 1, jnp.where(p < z, n_z, p)))
        at = ds(n, cut)
        return rc(
            part.at[p, ds(fy, quarter), at], z_in.at[slot, :, at],
            zi_ss.at[p, n], zi_rs.at[slot, n], plane(to),
        )

    def zi_wait(slot, n):
        dst = z_in.at[slot, :, ds(n, cut)]
        rc(dst, dst, zi_ss.at[0, n], zi_rs.at[slot, n], partner).wait_recv()

    def sweep(p):
        @pl.loop(0, half // 32)
        def _(r):
            at = ds(p * (half // 32) + r, 32)
            to = ds(r, 32)
            gate_pre, up_pre, hidden_grad = pre[0, at], pre[1, at], pre[2, at]
            sig = jax.nn.sigmoid(gate_pre)
            silu = gate_pre * sig
            hidden_b[to] = (silu * up_pre).astype(BF16)
            gate_g[to] = (hidden_grad * up_pre * sig * (1.0 + gate_pre * (1.0 - sig))).astype(BF16)
            up_g[to] = (hidden_grad * silu).astype(BF16)

        @pl.loop(0, n_cut)
        def _(n):
            for k in range(n_tp // n_cut):
                m = n * (n_tp // n_cut) + k
                part[p, :, ds(m, cols)] = (
                    jnp.dot(gate_g[...], wts[0, m], preferred_element_type=F32)
                    + jnp.dot(up_g[...], wts[1, m], preferred_element_type=F32)
                ).astype(BF16)
            yi_copy(p, n).start()

        @pl.loop(0, 2)
        def _(n):
            at = ds(n, width // 2)
            acc[:, at] += contract_tokens(hidden_b[...], tok[1, ds(p, half), at])

    mine = ds(fy, quarter)

    def yi_wait(p, n):
        dst = y_in.at[p, :, ds(n, cut)]
        rc(dst, dst, yi_ss.at[p, n], yi_rs.at[p, n], dev_y).wait_recv()

    def y_add(p):
        up = jnp.where(p > z, z - 1, z + 1)
        more = (up >= 0) & (up < n_z) & (up // (n_z // 2) == top)

        @pl.loop(0, n_cut)
        def _(n):
            at = ds(n, cut)
            yi_wait(p, n)
            total = part[p, mine, at].astype(F32) + y_in[p, :, at].astype(F32)
            part[p, mine, at] = total.astype(BF16)

            @pl.when(more)
            def _():
                zi_wait(p, n)
                part[p, mine, at] = (total + z_in[p, :, at].astype(F32)).astype(BF16)

            zi_copy(p, n).start()

    def far(k):
        return jnp.where(k == n_z - 1, z, near(n_z - 1 - k))

    outer = (z == 0) | (z == n_z - 1)

    @pl.loop(0, n_z)
    def _(j):
        sweep(far(j))

        @pl.when((j == n_z - 2) & outer)
        def _():
            y_add(far(0))

    def dn_copy(p):
        return rc(dn_out.at[p], dn_in.at[p], dn_ss.at[p], dn_rs.at[p], partner)

    def dx_copy(p):
        return rc(dx_out.at[p], dx_in.at[p], dx_ss.at[p], dx_rs.at[p], dev_x)

    def dz_copy(p):
        return rc(dz_out.at[p], dz_in.at[z], dz_ss.at[p], dz_rs.at[z], plane(p))

    @pl.loop(0, n_z)
    def _(k):
        p = far(k)
        dn_out[p] = acc[:, ds(p * 2 + 1 - c, cols)].astype(BF16)
        dn_copy(p).start()

    @pl.loop(0, n_z)
    def _(k):
        p = far(k)
        dn_copy(p).wait_recv()
        mine = ds(p * 2 + c, cols)
        other = ds(1 - fx, hid)
        here = ds(fx, hid)
        dx_out[p] = (acc[other, mine] + dn_in[p, other].astype(F32)).astype(BF16)
        dx_copy(p).start()
        acc[here, mine] = acc[here, mine] + dn_in[p, here].astype(F32)

    def dx_add(p):
        dx_copy(p).wait_recv()
        total = acc[ds(fx, hid), ds(p * 2 + c, cols)] + dx_in[p].astype(F32)

        @pl.when(p == z)
        def _():
            down_ref[ds(z, hid)] = total

        @pl.when(p != z)
        def _():
            dz_out[p] = total.astype(BF16)
            dz_copy(p).start()

    y_add(far(1))

    @pl.when(jnp.logical_not(outer))
    def _():
        y_add(far(0))

    for k in range(2, n_z - 1):
        y_add(far(k))
    for k in range(n_z - 1):
        dx_add(far(k))

    own_rows = ds(fx * 2 + fy, quarter)
    x_rows = ds((1 - fx) * 2 + fy, quarter)
    y_rows = ds(fx * 2 + 1 - fy, quarter)
    d_rows = ds((1 - fx) * 2 + 1 - fy, quarter)

    def ag_copy(i, n, rows, dev):
        src = grad_ref.at[0, rows, ds(n, cut)]
        return rc(src, src, ag_ss.at[i, n], ag_rs.at[i, n], dev)

    below = (z > 0) & ((z - 1) // (n_z // 2) == top)
    above = (z < n_z - 1) & ((z + 1) // (n_z // 2) == top)

    @pl.loop(0, n_cut)
    def _(n):
        at = ds(n, cut)

        def gain(slot):
            zi_wait(slot, n)
            total[...] += z_in[slot, :, at].astype(F32)

        yi_wait(z, n)
        total[...] = part[z, mine, at].astype(F32) + y_in[z, :, at].astype(F32)
        gain(n_z + 1)
        pl.when(below)(lambda: gain(z))
        pl.when(above)(lambda: gain(n_z))
        grad_ref[0, own_rows, at] = total[...].astype(BF16)
        ag_copy(1, n, own_rows, dev_y).start()
        ag_copy(0, n, own_rows, dev_x).start()

    dx_add(z)

    @pl.loop(0, n_cut)
    def _(n):
        ag_copy(1, n, y_rows, dev_y).wait_recv()
        ag_copy(2, n, y_rows, dev_x).start()

    for j in range(1, n_z):
        s = near(j)
        dst = dz_in.at[s]
        rc(dst, dst, dz_ss.at[s], dz_rs.at[s], partner).wait_recv()
        down_ref[ds(s, hid)] = dz_in[s].astype(F32)

    for n in range(n_cut):
        ag_copy(0, n, x_rows, dev_x).wait_recv()
        ag_copy(2, n, d_rows, dev_x).wait_recv()

    for arr in range(2):
        for p in range(n_z):
            @pl.when((z < n_z - 1) & (p <= z))
            def _(arr=arr, p=p):
                z_copy(arr, p, 1).wait_send()

            @pl.when((z > 0) & (p >= z))
            def _(arr=arr, p=p):
                z_copy(arr, p, 0).wait_send()

            @pl.when(p != z)
            def _(arr=arr, p=p):
                y_copy(arr, p).wait_send()

    for p in range(n_z):
        for i in range(3):
            x_copy(i, p).wait_send()
            d_copy(i, 0, p).wait_send()
            d_copy(i, 1, p).wait_send()
        for n in range(n_cut):
            yi_copy(p, n).wait_send()
        dn_copy(p).wait_send()
        dx_copy(p).wait_send()

        @pl.when(p != z)
        def _(p=p):
            for n in range(n_cut):
                zi_copy(p, n).wait_send()
            dz_copy(p).wait_send()

    for s in range(n_z):
        for to in range(n_z):
            if s == to:
                continue

            @pl.when((z >= s) & (z < to) if s < to else (z <= s) & (z > to))
            def _(s=s, to=to):
                for i in range(3):
                    src = fwd.at[i, s, to]
                    rc(src, src, w_ss.at[i, s, to], w_rs.at[i, s, to], partner).wait_send()

    for n in range(n_cut):
        ag_copy(0, n, own_rows, dev_x).wait_send()
        ag_copy(1, n, own_rows, dev_y).wait_send()
        ag_copy(2, n, y_rows, dev_x).wait_send()


def spread(n_tp, inputs, cotangent, gate_weight, up_weight, down_weight):
    _, n_tok, width = inputs.shape
    hid_all = gate_weight.shape[1]
    n_z = n_tp // 2
    hid, cols, half, quarter = hid_all // n_z, width // n_tp, n_tok // 2, n_tok // 4
    dma = pltpu.SemaphoreType.DMA
    vmem = pl.BlockSpec(memory_space=pltpu.VMEM)
    anyspace = pl.BlockSpec(memory_space=pl.ANY)
    return pl.pallas_call(
        functools.partial(kernel, n_tp),
        name="spread_hidden",
        out_shape=(
            jax.ShapeDtypeStruct((1, n_tok, width), BF16),
            jax.ShapeDtypeStruct((hid_all, cols), F32),
        ),
        in_specs=[anyspace, anyspace, vmem, vmem, vmem],
        out_specs=(vmem, vmem),
        scratch_shapes=[
            pltpu.VMEM((2, n_z * half, width), BF16),
            pltpu.VMEM((3, n_tp, 2 * hid, cols), BF16),
            pltpu.VMEM((hid_all, cols), BF16),
            pltpu.VMEM((hid_all, cols), BF16),
            pltpu.VMEM((n_z, half, width), BF16),
            pltpu.VMEM((n_z, quarter, width), BF16),
            pltpu.VMEM((n_z + 2, quarter, width), BF16),
            pltpu.VMEM((2 * hid, width), F32),
            pltpu.VMEM((3, n_z * half, 2 * hid), F32),
            pltpu.VMEM((half, 2 * hid), BF16),
            pltpu.VMEM((half, 2 * hid), BF16),
            pltpu.VMEM((half, 2 * hid), BF16),
            pltpu.VMEM((quarter, width // 4), F32),
            pltpu.VMEM((n_z, 2 * hid, cols), BF16),
            pltpu.VMEM((n_z, 2 * hid, cols), BF16),
            pltpu.VMEM((n_z, hid, cols), BF16),
            pltpu.VMEM((n_z, hid, cols), BF16),
            pltpu.VMEM((n_z, hid, cols), BF16),
            pltpu.VMEM((n_z, hid, cols), BF16),
            pltpu.VMEM((3, n_z, n_z, hid, cols), BF16),
            dma((2,)), dma((2, n_z, 2)), dma((2, n_z)), dma((2, n_z)), dma((2, n_z)),
            dma((3, n_z, n_z)), dma((3, n_z, n_z)), dma((3, n_z)), dma((3, n_z)),
            dma((3, 2, n_z)), dma((3, 2, n_z)),
            dma((n_z, 4)), dma((n_z, 4)), dma((n_z, 4)), dma((n_z + 2, 4)), dma((3, 4)), dma((3, 4)),
            dma((n_z,)), dma((n_z,)), dma((n_z,)), dma((n_z,)), dma((n_z,)), dma((n_z,)),
        ],
        compiler_params=pltpu.CompilerParams(
            collective_id=0, has_side_effects=True, vmem_limit_bytes=66_000_000
        ),
    )(inputs, cotangent, gate_weight, up_weight, down_weight)


def solution(mesh):
    n_fs, n_tp = mesh.shape["fs"], mesh.shape["tp"]

    def per_device(inputs, cotangent, gate_weight, up_weight, down_weight):
        _, n_tok, width = inputs.shape
        hid_all = gate_weight.shape[1]
        n_z = n_tp // 2
        fits = (
            n_fs == 4
            and n_tp % 2 == 0
            and hid_all % (n_z * 16) == 0
            and width % (n_tp * 128) == 0
            and n_tok % 64 == 0
            and (3 * n_tok + 9 * hid_all) * n_z * width + 18 * hid_all * width < 62_000_000 * n_z
        )
        if not fits:
            return gathered(inputs, cotangent, gate_weight, up_weight, down_weight)
        return spread(n_tp, inputs, cotangent, gate_weight, up_weight, down_weight)

    return jax.shard_map(
        per_device,
        mesh=mesh,
        in_specs=(
            P("tp", None, None),
            P("tp", None, None),
            P("tp", "fs"),
            P("tp", "fs"),
            P("fs", "tp"),
        ),
        out_specs=(P("tp", None, None), P("fs", "tp")),
        check_vma=False,
    )
```

```python
import functools

import jax
import jax.numpy as jnp
from jax import lax
from jax.experimental import pallas as pl
from jax.experimental.pallas import tpu as pltpu
from jax.sharding import PartitionSpec as P

MESH = pl.DeviceIdType.MESH
BF16 = jnp.bfloat16
F32 = jnp.float32


def contract_hidden(left, right):
    return lax.dot_general(left, right, (((1,), (1,)), ((), ())), preferred_element_type=F32)


def contract_tokens(left, right):
    return lax.dot_general(left, right, (((0,), (0,)), ((), ())), preferred_element_type=F32)


def gathered(inputs, cotangent, gate_weight, up_weight, down_weight):
    rows_in = inputs[0]
    rows_grad = cotangent[0]
    token_count, model_width = rows_in.shape
    gate_full = lax.all_gather(gate_weight, "tp", axis=0, tiled=True)
    up_full = lax.all_gather(up_weight, "tp", axis=0, tiled=True)
    down_tall = lax.all_gather(down_weight.T, "tp", axis=0, tiled=True)
    gate_pre = jnp.dot(rows_in, gate_full, preferred_element_type=F32)
    up_pre = jnp.dot(rows_in, up_full, preferred_element_type=F32)
    sig = jax.nn.sigmoid(gate_pre)
    hidden = (gate_pre * sig * up_pre).astype(BF16)
    hidden_grad = jnp.dot(rows_grad, down_tall, preferred_element_type=F32)
    gate_grad = (hidden_grad * up_pre * sig * (1.0 + gate_pre * (1.0 - sig))).astype(BF16)
    up_grad = (hidden_grad * gate_pre * sig).astype(BF16)
    partial_down = contract_tokens(hidden, rows_grad)
    down_grad = lax.psum_scatter(
        partial_down.astype(BF16), "tp", scatter_dimension=1, tiled=True
    ).astype(F32)
    own_sum = lax.psum_scatter(
        (contract_hidden(gate_grad, gate_full) + contract_hidden(up_grad, up_full)).astype(BF16),
        "fs",
        scatter_dimension=0,
        tiled=True,
    )
    whole_grad = lax.all_gather(own_sum, "fs", axis=0, tiled=True)
    return (whole_grad.reshape(1, token_count, model_width), down_grad)


def kernel(
    n_tp, x_ref, ct_ref, wg_hbm, wu_hbm, wd_hbm, grad_hbm, down_hbm,
    wg_ref, wu_ref, wd_ref, grad_ref, down_ref,
    tok, wts, gate_t, up_t, part, y_in, z_in, acc, pre, gate_g, up_g, hidden_b, total,
    dn_out, dn_in, dx_out, dx_in, dz_out, dz_in, fwd,
    loc_sem, out_sem, z_ss, y_ss, tok_zs, tok_ys, w_ss, w_rs, x_ss, x_rs, d_ss, d_rs,
    yi_ss, yi_rs, zi_ss, zi_rs, ag_ss, ag_rs, dn_ss, dn_rs, dx_ss, dx_rs, dz_ss, dz_rs,
):
    f, t = lax.axis_index("fs"), lax.axis_index("tp")
    n_z = n_tp // 2
    z, c = t // 2, t % 2
    fy, fx = f // 2, f % 2
    dev_x, dev_y = {"fs": fy * 2 + 1 - fx}, {"fs": (1 - fy) * 2 + fx}
    partner = {"tp": z * 2 + 1 - c}
    half, width = tok.shape[1] // n_z, tok.shape[2]
    quarter = half // 2
    hid = wts.shape[2] // 2
    cols = width // n_tp
    weights = (gate_t, up_t, wd_ref)

    def plane(p):
        return {"tp": p * 2 + c}

    def rc(src, dst, ss, rs, dev):
        return pltpu.make_async_remote_copy(
            src_ref=src, dst_ref=dst, send_sem=ss, recv_sem=rs, device_id=dev, device_id_type=MESH
        )

    def ds(index, size):
        return pl.ds(pl.multiple_of(index * size, size), size)

    def near(j):
        low = jnp.where(z < n_z // 2, z, n_z - 1 - z)
        step = jnp.where(j % 2 == 1, (j + 1) // 2, -(j // 2))
        p = jnp.where(j <= 2 * low, low + step, j)
        return jnp.where(z < n_z // 2, p, n_z - 1 - p)

    def tok_rows(arr, p, side):
        start = pl.multiple_of(p * half + side * quarter, quarter)
        return tok.at[arr, pl.ds(start, quarter)]

    def z_copy(arr, p, d):
        src = tok_rows(arr, p, fy)
        to = z + 1 if d else z - 1
        return rc(src, src, z_ss.at[arr, p, d], tok_zs.at[arr, p], plane(to))

    def y_copy(arr, p):
        src = tok_rows(arr, p, fy)
        return rc(src, src, y_ss.at[arr, p], tok_ys.at[arr, p], dev_y)

    def z_tok_wait(arr, p):
        dst = tok_rows(arr, p, fy)
        rc(dst, dst, y_ss.at[arr, p], tok_zs.at[arr, p], dev_y).wait_recv()

    def y_tok_wait(arr, p):
        dst = tok_rows(arr, p, 1 - fy)
        rc(dst, dst, y_ss.at[arr, p], tok_ys.at[arr, p], dev_y).wait_recv()

    def tok_in(arr, p):
        z_tok_wait(arr, p)

        @pl.when((p < z) & (z < n_z - 1))
        def _():
            z_copy(arr, p, 1).start()

        @pl.when((p > z) & (z > 0))
        def _():
            z_copy(arr, p, 0).start()

        y_copy(arr, p).start()

    def block(i, side, s, core):
        return wts.at[i, s * 2 + core, ds(side, hid)]

    def own_block(i, p):
        return weights[i].at[ds(p, hid)]

    def w_wait(i, s, to):
        dst = fwd.at[i, s, to]
        rc(dst, dst, w_ss.at[i, s, to], w_rs.at[i, s, to], partner).wait_recv()

    def w_hop(i, s, to, src):
        via = jnp.where(to > z, z + 1, z - 1)
        sems = (w_ss.at[i, s, to], w_rs.at[i, s, to], plane(via))

        @pl.when(via == to)
        def _():
            rc(src, block(i, fx, s, c), *sems).start()

        @pl.when(via != to)
        def _():
            rc(src, fwd.at[i, s, to], *sems).start()

    def x_copy(i, s, src=None):
        dst = block(i, fx, s, c)
        return rc(dst if src is None else src, dst, x_ss.at[i, s], x_rs.at[i, s], dev_x)

    def d_copy(i, other, s, src=None):
        side = 1 - fx if other else fx
        dst = block(i, side, s, c)
        return rc(
            dst if src is None else src, dst, d_ss.at[i, other, s], d_rs.at[i, other, s], partner
        )

    own = [
        pltpu.make_async_copy(x_ref.at[0, ds(fx, half)], tok.at[0, ds(z, half)], loc_sem.at[0]),
        pltpu.make_async_copy(ct_ref.at[0, ds(fx, half)], tok.at[1, ds(z, half)], loc_sem.at[1]),
    ]
    load = [
        pltpu.make_async_copy(wd_hbm, wd_ref, loc_sem.at[2]),
        pltpu.make_async_copy(wg_hbm, wg_ref, loc_sem.at[3]),
        pltpu.make_async_copy(wu_hbm, wu_ref, loc_sem.at[4]),
    ]
    for copy in own + load:
        copy.start()

    barrier = pltpu.get_barrier_semaphore()
    for dev in (dev_x, dev_y):
        pl.semaphore_signal(barrier, inc=1, device_id=dev, device_id_type=MESH)
    for k in range(1, n_tp):
        pl.semaphore_signal(barrier, inc=1, device_id={"tp": (t + k) % n_tp}, device_id_type=MESH)
    pl.semaphore_wait(barrier, 2 + n_tp - 1)

    for arr in range(2):
        own[arr].wait()
        for d, ok in ((1, z < n_z - 1), (0, z > 0)):
            @pl.when(ok)
            def _(arr=arr, d=d):
                z_copy(arr, z, d).start()

    order_i = (2, 0, 1)

    def w_own(i):
        x_copy(i, z, own_block(i, z)).start()
        d_copy(i, 0, z, own_block(i, z)).start()
        for e in range(1, n_z):
            for to, ok in ((z + e, z + e < n_z), (z - e, z >= e)):
                if e == 1:
                    @pl.when(ok)
                    def _(to=to):
                        w_hop(i, z, to, own_block(i, to))

    load[0].wait()
    w_own(2)
    load[1].wait()
    gate_t[...] = wg_ref[...].T
    w_own(0)
    load[2].wait()
    up_t[...] = wu_ref[...].T
    w_own(1)
    for e in range(n_z - 1, 1, -1):
        for i in order_i:
            for to, ok in ((z + e, z + e < n_z), (z - e, z >= e)):
                @pl.when(ok)
                def _(i=i, to=to):
                    w_hop(i, z, to, own_block(i, to))
    for i in range(3):
        wts[i, t, ds(fx, hid)] = weights[i][ds(z, hid)]
    acc[...] = jnp.zeros_like(acc)
    pre[...] = jnp.zeros_like(pre)

    def sides(g):
        return ((z - g, z >= g, 1), (z + g, z + g < n_z, -1))

    def w_in(i, s):
        w_wait(i, s, z)
        x_copy(i, s).start()
        d_copy(i, 0, s).start()

    last = jnp.where(z < n_z // 2, n_z - 1, 0)

    def x_in(i, s):
        dst = block(i, 1 - fx, s, c)
        rc(dst, dst, x_ss.at[i, s], x_rs.at[i, s], partner).wait_recv()
        d_copy(i, 1, s).start()

    def unit(p, s):
        rows = ds(p, half)
        for i in range(3):
            total = pre[i, rows]
            for k in range(2):
                at = ds(s * 2 + k, cols)
                total += contract_hidden(tok[1 if i == 2 else 0, rows, at], wts[i, s * 2 + k])
            pre[i, rows] = total

    def arrived(i, s):
        for other in range(2):
            side = 1 - fx if other else fx
            dst = block(i, side, s, 1 - c)
            rc(dst, dst, d_ss.at[i, other, s], d_rs.at[i, other, s], partner).wait_recv()

    def finish(g):
        for k, (s, ok, _) in enumerate(sides(g)):
            @pl.when(ok & (s != last))
            def _(k=k, s=s):
                for i in order_i:
                    x_in(i, s)
                for arr in range(2):
                    y_tok_wait(arr, s)
                for i in order_i:
                    arrived(i, s)
                unit(s, s)

                @pl.loop(0, n_z)
                def _(r):
                    dist = jnp.where(r > z, r - z, z - r)
                    known = dist < g
                    if k == 1:
                        known = known | (r == z - g)

                    @pl.when(known)
                    def _():
                        unit(s, r)
                        unit(r, s)

    def w_group(g):
        for i in order_i:
            for s, ok, _ in sides(g):
                @pl.when(ok)
                def _(i=i, s=s):
                    w_in(i, s)

    def w_pass(g):
        for q in range(n_z - g, 0, -1):
            for i in order_i:
                for k, (s, ok, step) in enumerate(sides(g)):
                    e = jnp.where(z // (n_z // 2) == k, q, q - 1)
                    to = z + step * e

                    @pl.when(ok & (e > 0) & (to >= 0) & (to < n_z))
                    def _(i=i, s=s, to=to):
                        w_wait(i, s, to)
                        w_hop(i, s, to, fwd.at[i, s, to])

    for g in range(1, n_z):
        for arr in range(2):
            for s, ok, _ in sides(g):
                @pl.when(ok)
                def _(arr=arr, s=s):
                    tok_in(arr, s)
        if g == 1:
            for i in order_i:
                x_in(i, z)
                arrived(i, z)
            unit(z, z)
        else:
            finish(g - 1)
        if g == 1:
            w_group(g)
            w_pass(g)
        else:
            w_pass(g)
            w_group(g)

    for arr in range(2):
        y_tok_wait(arr, last)

    @pl.loop(0, n_z)
    def _(r):
        @pl.when(r != last)
        def _():
            unit(last, r)

    def whole(i):
        arrived(i, last)

        @pl.loop(0, n_z // 2)
        def _(m):
            rows = ds(m, 2 * half)
            total = pre[i, rows]
            for k in range(2):
                at = ds(last * 2 + k, cols)
                total += contract_hidden(tok[1 if i == 2 else 0, rows, at], wts[i, last * 2 + k])
            pre[i, rows] = total

    x_in(2, last)
    x_in(0, last)
    whole(2)
    whole(0)
    x_in(1, last)
    whole(1)

    n_cut = 2
    cut = width // n_cut

    def yi_copy(p, n):
        at = ds(n, cut)
        return rc(
            part.at[p, ds(1 - fy, quarter), at], y_in.at[p, :, at],
            yi_ss.at[p, n], yi_rs.at[p, n], dev_y,
        )

    top = z // (n_z // 2)

    def zi_copy(p, n):
        away = p // (n_z // 2) != top
        step = jnp.where(p > z, z + 1, z - 1)
        to = jnp.where(away & (step // (n_z // 2) != top), p, step)
        slot = jnp.where(to != p, p, jnp.where(away, n_z + 1, jnp.where(p < z, n_z, p)))
        at = ds(n, cut)
        return rc(
            part.at[p, ds(fy, quarter), at], z_in.at[slot, :, at],
            zi_ss.at[p, n], zi_rs.at[slot, n], plane(to),
        )

    def zi_wait(slot, n):
        dst = z_in.at[slot, :, ds(n, cut)]
        rc(dst, dst, zi_ss.at[0, n], zi_rs.at[slot, n], partner).wait_recv()

    def sweep(p):
        @pl.loop(0, half // 32)
        def _(r):
            at = ds(p * (half // 32) + r, 32)
            to = ds(r, 32)
            gate_pre, up_pre, hidden_grad = pre[0, at], pre[1, at], pre[2, at]
            sig = jax.nn.sigmoid(gate_pre)
            silu = gate_pre * sig
            hidden_b[to] = (silu * up_pre).astype(BF16)
            gate_g[to] = (hidden_grad * up_pre * sig * (1.0 + gate_pre * (1.0 - sig))).astype(BF16)
            up_g[to] = (hidden_grad * silu).astype(BF16)

        @pl.loop(0, n_cut)
        def _(n):
            for k in range(n_tp // n_cut):
                m = n * (n_tp // n_cut) + k
                part[p, :, ds(m, cols)] = (
                    jnp.dot(gate_g[...], wts[0, m], preferred_element_type=F32)
                    + jnp.dot(up_g[...], wts[1, m], preferred_element_type=F32)
                ).astype(BF16)
            yi_copy(p, n).start()

        @pl.loop(0, 2)
        def _(n):
            at = ds(n, width // 2)
            acc[:, at] += contract_tokens(hidden_b[...], tok[1, ds(p, half), at])

    mine = ds(fy, quarter)

    def yi_wait(p, n):
        dst = y_in.at[p, :, ds(n, cut)]
        rc(dst, dst, yi_ss.at[p, n], yi_rs.at[p, n], dev_y).wait_recv()

    def y_add(p):
        up = jnp.where(p > z, z - 1, z + 1)
        more = (up >= 0) & (up < n_z) & (up // (n_z // 2) == top)

        @pl.loop(0, n_cut)
        def _(n):
            at = ds(n, cut)
            yi_wait(p, n)
            total = part[p, mine, at].astype(F32) + y_in[p, :, at].astype(F32)
            part[p, mine, at] = total.astype(BF16)

            @pl.when(more)
            def _():
                zi_wait(p, n)
                part[p, mine, at] = (total + z_in[p, :, at].astype(F32)).astype(BF16)

            zi_copy(p, n).start()

    def far(k):
        return jnp.where(k == n_z - 1, z, near(n_z - 1 - k))

    outer = (z == 0) | (z == n_z - 1)

    @pl.loop(0, n_z)
    def _(j):
        sweep(far(j))

        @pl.when((j == n_z - 2) & outer)
        def _():
            y_add(far(0))

    def dn_copy(p):
        return rc(dn_out.at[p], dn_in.at[p], dn_ss.at[p], dn_rs.at[p], partner)

    def dx_copy(p):
        return rc(dx_out.at[p], dx_in.at[p], dx_ss.at[p], dx_rs.at[p], dev_x)

    def dz_copy(p):
        return rc(dz_out.at[p], dz_in.at[z], dz_ss.at[p], dz_rs.at[z], plane(p))

    @pl.loop(0, n_z)
    def _(k):
        p = far(k)
        dn_out[p] = acc[:, ds(p * 2 + 1 - c, cols)].astype(BF16)
        dn_copy(p).start()

    @pl.loop(0, n_z)
    def _(k):
        p = far(k)
        dn_copy(p).wait_recv()
        mine = ds(p * 2 + c, cols)
        other = ds(1 - fx, hid)
        here = ds(fx, hid)
        dx_out[p] = (acc[other, mine] + dn_in[p, other].astype(F32)).astype(BF16)
        dx_copy(p).start()
        acc[here, mine] = acc[here, mine] + dn_in[p, here].astype(F32)

    def down_out(p):
        rows = ds(p, hid)
        return pltpu.make_async_copy(down_ref.at[rows], down_hbm.at[rows], out_sem.at[p])

    def grad_out(i, rows):
        return pltpu.make_async_copy(grad_ref.at[rows], grad_hbm.at[0, rows], out_sem.at[n_z + i])

    def dx_add(p):
        dx_copy(p).wait_recv()
        total = acc[ds(fx, hid), ds(p * 2 + c, cols)] + dx_in[p].astype(F32)

        @pl.when(p == z)
        def _():
            down_ref[ds(z, hid)] = total
            down_out(z).start()

        @pl.when(p != z)
        def _():
            dz_out[p] = total.astype(BF16)
            dz_copy(p).start()

    y_add(far(1))

    @pl.when(jnp.logical_not(outer))
    def _():
        y_add(far(0))

    for k in range(2, n_z - 1):
        y_add(far(k))
    for k in range(n_z - 2):
        dx_add(far(k))

    own_rows = ds(fx * 2 + fy, quarter)
    x_rows = ds((1 - fx) * 2 + fy, quarter)
    y_rows = ds(fx * 2 + 1 - fy, quarter)
    d_rows = ds((1 - fx) * 2 + 1 - fy, quarter)

    def ag_copy(i, n, rows, dev):
        src = grad_ref.at[rows, ds(n, cut)]
        return rc(src, src, ag_ss.at[i, n], ag_rs.at[i, n], dev)

    below = (z > 0) & ((z - 1) // (n_z // 2) == top)
    above = (z < n_z - 1) & ((z + 1) // (n_z // 2) == top)

    @pl.loop(0, n_cut)
    def _(n):
        at = ds(n, cut)

        def gain(slot):
            zi_wait(slot, n)
            total[...] += z_in[slot, :, at].astype(F32)

        yi_wait(z, n)
        total[...] = part[z, mine, at].astype(F32) + y_in[z, :, at].astype(F32)
        gain(n_z + 1)
        pl.when(below)(lambda: gain(z))
        pl.when(above)(lambda: gain(n_z))
        grad_ref[own_rows, at] = total[...].astype(BF16)
        ag_copy(1, n, own_rows, dev_y).start()
        ag_copy(0, n, own_rows, dev_x).start()

    dx_add(far(n_z - 2))

    @pl.loop(0, n_cut)
    def _(n):
        ag_copy(1, n, y_rows, dev_y).wait_recv()
        ag_copy(2, n, y_rows, dev_x).start()

    dx_add(z)

    for j in range(1, n_z):
        s = near(j)
        dst = dz_in.at[s]
        rc(dst, dst, dz_ss.at[s], dz_rs.at[s], partner).wait_recv()
        down_ref[ds(s, hid)] = dz_in[s].astype(F32)
        down_out(s).start()

    grad_out(0, own_rows).start()
    grad_out(1, y_rows).start()
    for n in range(n_cut):
        ag_copy(0, n, x_rows, dev_x).wait_recv()
    grad_out(2, x_rows).start()
    for n in range(n_cut):
        ag_copy(2, n, d_rows, dev_x).wait_recv()
    grad_out(3, d_rows).start()

    for arr in range(2):
        for p in range(n_z):
            @pl.when((z < n_z - 1) & (p <= z))
            def _(arr=arr, p=p):
                z_copy(arr, p, 1).wait_send()

            @pl.when((z > 0) & (p >= z))
            def _(arr=arr, p=p):
                z_copy(arr, p, 0).wait_send()

            @pl.when(p != z)
            def _(arr=arr, p=p):
                y_copy(arr, p).wait_send()

    for p in range(n_z):
        for i in range(3):
            x_copy(i, p).wait_send()
            d_copy(i, 0, p).wait_send()
            d_copy(i, 1, p).wait_send()
        for n in range(n_cut):
            yi_copy(p, n).wait_send()
        dn_copy(p).wait_send()
        dx_copy(p).wait_send()

        @pl.when(p != z)
        def _(p=p):
            for n in range(n_cut):
                zi_copy(p, n).wait_send()
            dz_copy(p).wait_send()

    for s in range(n_z):
        for to in range(n_z):
            if s == to:
                continue

            @pl.when((z >= s) & (z < to) if s < to else (z <= s) & (z > to))
            def _(s=s, to=to):
                for i in range(3):
                    src = fwd.at[i, s, to]
                    rc(src, src, w_ss.at[i, s, to], w_rs.at[i, s, to], partner).wait_send()

    for n in range(n_cut):
        ag_copy(0, n, own_rows, dev_x).wait_send()
        ag_copy(1, n, own_rows, dev_y).wait_send()
        ag_copy(2, n, y_rows, dev_x).wait_send()
    for p in range(n_z):
        down_out(p).wait()
    for i, rows in enumerate((own_rows, y_rows, x_rows, d_rows)):
        grad_out(i, rows).wait()


def spread(n_tp, inputs, cotangent, gate_weight, up_weight, down_weight):
    _, n_tok, width = inputs.shape
    hid_all = gate_weight.shape[1]
    n_z = n_tp // 2
    hid, cols, half, quarter = hid_all // n_z, width // n_tp, n_tok // 2, n_tok // 4
    dma = pltpu.SemaphoreType.DMA
    anyspace = pl.BlockSpec(memory_space=pl.ANY)
    return pl.pallas_call(
        functools.partial(kernel, n_tp),
        name="spread_hidden",
        out_shape=(
            jax.ShapeDtypeStruct((1, n_tok, width), BF16),
            jax.ShapeDtypeStruct((hid_all, cols), F32),
        ),
        in_specs=[anyspace] * 5,
        out_specs=(anyspace, anyspace),
        scratch_shapes=[
            pltpu.VMEM(gate_weight.shape, BF16),
            pltpu.VMEM(up_weight.shape, BF16),
            pltpu.VMEM(down_weight.shape, BF16),
            pltpu.VMEM((n_tok, width), BF16),
            pltpu.VMEM((hid_all, cols), F32),
            pltpu.VMEM((2, n_z * half, width), BF16),
            pltpu.VMEM((3, n_tp, 2 * hid, cols), BF16),
            pltpu.VMEM((hid_all, cols), BF16),
            pltpu.VMEM((hid_all, cols), BF16),
            pltpu.VMEM((n_z, half, width), BF16),
            pltpu.VMEM((n_z, quarter, width), BF16),
            pltpu.VMEM((n_z + 2, quarter, width), BF16),
            pltpu.VMEM((2 * hid, width), F32),
            pltpu.VMEM((3, n_z * half, 2 * hid), F32),
            pltpu.VMEM((half, 2 * hid), BF16),
            pltpu.VMEM((half, 2 * hid), BF16),
            pltpu.VMEM((half, 2 * hid), BF16),
            pltpu.VMEM((quarter, width // 2), F32),
            pltpu.VMEM((n_z, 2 * hid, cols), BF16),
            pltpu.VMEM((n_z, 2 * hid, cols), BF16),
            pltpu.VMEM((n_z, hid, cols), BF16),
            pltpu.VMEM((n_z, hid, cols), BF16),
            pltpu.VMEM((n_z, hid, cols), BF16),
            pltpu.VMEM((n_z, hid, cols), BF16),
            pltpu.VMEM((3, n_z, n_z, hid, cols), BF16),
            dma((5,)), dma((n_z + 4,)), dma((2, n_z, 2)), dma((2, n_z)), dma((2, n_z)), dma((2, n_z)),
            dma((3, n_z, n_z)), dma((3, n_z, n_z)), dma((3, n_z)), dma((3, n_z)),
            dma((3, 2, n_z)), dma((3, 2, n_z)),
            dma((n_z, 2)), dma((n_z, 2)), dma((n_z, 2)), dma((n_z + 2, 2)), dma((3, 2)), dma((3, 2)),
            dma((n_z,)), dma((n_z,)), dma((n_z,)), dma((n_z,)), dma((n_z,)), dma((n_z,)),
        ],
        compiler_params=pltpu.CompilerParams(
            collective_id=0, has_side_effects=True, vmem_limit_bytes=66_000_000
        ),
    )(inputs, cotangent, gate_weight, up_weight, down_weight)


def solution(mesh):
    n_fs, n_tp = mesh.shape["fs"], mesh.shape["tp"]

    def per_device(inputs, cotangent, gate_weight, up_weight, down_weight):
        _, n_tok, width = inputs.shape
        hid_all = gate_weight.shape[1]
        n_z = n_tp // 2
        fits = (
            n_fs == 4
            and n_tp == 2 * n_z
            and hid_all % (n_z * 32) == 0
            and width % (n_tp * 128) == 0
            and n_tok % 64 == 0
            and (3 * n_tok + 9 * hid_all) * n_z * width + 18 * hid_all * width < 62_000_000 * n_z
        )
        if not fits:
            return gathered(inputs, cotangent, gate_weight, up_weight, down_weight)
        return spread(n_tp, inputs, cotangent, gate_weight, up_weight, down_weight)

    return jax.shard_map(
        per_device,
        mesh=mesh,
        in_specs=(
            P("tp", None, None),
            P("tp", None, None),
            P("tp", "fs"),
            P("tp", "fs"),
            P("fs", "tp"),
        ),
        out_specs=(P("tp", None, None), P("fs", "tp")),
        check_vma=False,
    )
```

```python
import functools

import jax
import jax.numpy as jnp
from jax import lax
from jax.experimental import pallas as pl
from jax.experimental.pallas import tpu as pltpu
from jax.sharding import PartitionSpec as P

MESH = pl.DeviceIdType.MESH
BF16 = jnp.bfloat16
F32 = jnp.float32


def contract_hidden(left, right):
    return lax.dot_general(left, right, (((1,), (1,)), ((), ())), preferred_element_type=F32)


def contract_tokens(left, right):
    return lax.dot_general(left, right, (((0,), (0,)), ((), ())), preferred_element_type=F32)


def gathered(inputs, cotangent, gate_weight, up_weight, down_weight):
    rows_in = inputs[0]
    rows_grad = cotangent[0]
    token_count, model_width = rows_in.shape
    gate_full = lax.all_gather(gate_weight, "tp", axis=0, tiled=True)
    up_full = lax.all_gather(up_weight, "tp", axis=0, tiled=True)
    down_tall = lax.all_gather(down_weight.T, "tp", axis=0, tiled=True)
    gate_pre = jnp.dot(rows_in, gate_full, preferred_element_type=F32)
    up_pre = jnp.dot(rows_in, up_full, preferred_element_type=F32)
    sig = jax.nn.sigmoid(gate_pre)
    hidden = (gate_pre * sig * up_pre).astype(BF16)
    hidden_grad = jnp.dot(rows_grad, down_tall, preferred_element_type=F32)
    gate_grad = (hidden_grad * up_pre * sig * (1.0 + gate_pre * (1.0 - sig))).astype(BF16)
    up_grad = (hidden_grad * gate_pre * sig).astype(BF16)
    partial_down = contract_tokens(hidden, rows_grad)
    down_grad = lax.psum_scatter(
        partial_down.astype(BF16), "tp", scatter_dimension=1, tiled=True
    ).astype(F32)
    own_sum = lax.psum_scatter(
        (contract_hidden(gate_grad, gate_full) + contract_hidden(up_grad, up_full)).astype(BF16),
        "fs",
        scatter_dimension=0,
        tiled=True,
    )
    whole_grad = lax.all_gather(own_sum, "fs", axis=0, tiled=True)
    return (whole_grad.reshape(1, token_count, model_width), down_grad)


def kernel(
    n_tp, x_ref, ct_ref, wg_hbm, wu_hbm, wd_hbm, grad_hbm, down_hbm,
    wg_ref, wu_ref, wd_ref, grad_ref, down_ref,
    tok, wts, gate_t, up_t, part, y_in, z_in, acc, pre, gate_g, up_g, hidden_b, total,
    dn_out, dn_in, dx_out, dx_in, dz_out, dz_in, fwd,
    loc_sem, out_sem, z_ss, y_ss, tok_zs, tok_ys, w_ss, w_rs, x_ss, x_rs, d_ss, d_rs,
    yi_ss, yi_rs, zi_ss, zi_rs, ag_ss, ag_rs, dn_ss, dn_rs, dx_ss, dx_rs, dz_ss, dz_rs,
):
    f, t = lax.axis_index("fs"), lax.axis_index("tp")
    n_z = n_tp // 2
    z, c = t // 2, t % 2
    fy, fx = f // 2, f % 2
    dev_x, dev_y = {"fs": fy * 2 + 1 - fx}, {"fs": (1 - fy) * 2 + fx}
    partner = {"tp": z * 2 + 1 - c}
    half, width = tok.shape[1] // n_z, tok.shape[2]
    quarter = half // 2
    hid = wts.shape[2] // 2
    cols = width // n_tp
    weights = (gate_t, up_t, wd_ref)

    def plane(p):
        return {"tp": p * 2 + c}

    def rc(src, dst, ss, rs, dev):
        return pltpu.make_async_remote_copy(
            src_ref=src, dst_ref=dst, send_sem=ss, recv_sem=rs, device_id=dev, device_id_type=MESH
        )

    def ds(index, size):
        return pl.ds(pl.multiple_of(index * size, size), size)

    def near(j):
        low = jnp.where(z < n_z // 2, z, n_z - 1 - z)
        step = jnp.where(j % 2 == 1, (j + 1) // 2, -(j // 2))
        p = jnp.where(j <= 2 * low, low + step, j)
        return jnp.where(z < n_z // 2, p, n_z - 1 - p)

    def tok_rows(arr, p, side):
        start = pl.multiple_of(p * half + side * quarter, quarter)
        return tok.at[arr, pl.ds(start, quarter)]

    def z_copy(arr, p, d):
        src = tok_rows(arr, p, fy)
        to = z + 1 if d else z - 1
        return rc(src, src, z_ss.at[arr, p, d], tok_zs.at[arr, p], plane(to))

    def y_copy(arr, p):
        src = tok_rows(arr, p, fy)
        return rc(src, src, y_ss.at[arr, p], tok_ys.at[arr, p], dev_y)

    def z_tok_wait(arr, p):
        dst = tok_rows(arr, p, fy)
        rc(dst, dst, y_ss.at[arr, p], tok_zs.at[arr, p], dev_y).wait_recv()

    def y_tok_wait(arr, p):
        dst = tok_rows(arr, p, 1 - fy)
        rc(dst, dst, y_ss.at[arr, p], tok_ys.at[arr, p], dev_y).wait_recv()

    def tok_in(arr, p):
        z_tok_wait(arr, p)

        @pl.when((p < z) & (z < n_z - 1))
        def _():
            z_copy(arr, p, 1).start()

        @pl.when((p > z) & (z > 0))
        def _():
            z_copy(arr, p, 0).start()

        y_copy(arr, p).start()

    def block(i, side, s, core):
        return wts.at[i, s * 2 + core, ds(side, hid)]

    def own_block(i, p):
        return weights[i].at[ds(p, hid)]

    def w_wait(i, s, to):
        dst = fwd.at[i, s, to]
        rc(dst, dst, w_ss.at[i, s, to], w_rs.at[i, s, to], partner).wait_recv()

    def w_hop(i, s, to, src):
        via = jnp.where(to > z, z + 1, z - 1)
        sems = (w_ss.at[i, s, to], w_rs.at[i, s, to], plane(via))

        @pl.when(via == to)
        def _():
            rc(src, block(i, fx, s, c), *sems).start()

        @pl.when(via != to)
        def _():
            rc(src, fwd.at[i, s, to], *sems).start()

    def x_copy(i, s, src=None):
        dst = block(i, fx, s, c)
        return rc(dst if src is None else src, dst, x_ss.at[i, s], x_rs.at[i, s], dev_x)

    def d_copy(i, other, s, src=None):
        side = 1 - fx if other else fx
        dst = block(i, side, s, c)
        return rc(
            dst if src is None else src, dst, d_ss.at[i, other, s], d_rs.at[i, other, s], partner
        )

    own = [
        pltpu.make_async_copy(x_ref.at[0, ds(fx, half)], tok.at[0, ds(z, half)], loc_sem.at[0]),
        pltpu.make_async_copy(ct_ref.at[0, ds(fx, half)], tok.at[1, ds(z, half)], loc_sem.at[1]),
    ]
    load = [
        pltpu.make_async_copy(wd_hbm, wd_ref, loc_sem.at[2]),
        pltpu.make_async_copy(wg_hbm, wg_ref, loc_sem.at[3]),
        pltpu.make_async_copy(wu_hbm, wu_ref, loc_sem.at[4]),
    ]
    for copy in own + load:
        copy.start()

    barrier = pltpu.get_barrier_semaphore()
    for dev in (dev_x, dev_y):
        pl.semaphore_signal(barrier, inc=1, device_id=dev, device_id_type=MESH)
    for k in range(1, n_tp):
        pl.semaphore_signal(barrier, inc=1, device_id={"tp": (t + k) % n_tp}, device_id_type=MESH)
    pl.semaphore_wait(barrier, 2 + n_tp - 1)

    for arr in range(2):
        own[arr].wait()
        for d, ok in ((1, z < n_z - 1), (0, z > 0)):
            @pl.when(ok)
            def _(arr=arr, d=d):
                z_copy(arr, z, d).start()

    order_i = (2, 0, 1)

    def w_own(i):
        x_copy(i, z, own_block(i, z)).start()
        d_copy(i, 0, z, own_block(i, z)).start()
        for e in range(1, n_z):
            for to, ok in ((z + e, z + e < n_z), (z - e, z >= e)):
                if e == 1:
                    @pl.when(ok)
                    def _(to=to):
                        w_hop(i, z, to, own_block(i, to))

    load[0].wait()
    w_own(2)
    load[1].wait()
    gate_t[...] = wg_ref[...].T
    w_own(0)
    load[2].wait()
    up_t[...] = wu_ref[...].T
    w_own(1)
    for e in range(n_z - 1, 1, -1):
        for i in order_i:
            for to, ok in ((z + e, z + e < n_z), (z - e, z >= e)):
                @pl.when(ok)
                def _(i=i, to=to):
                    w_hop(i, z, to, own_block(i, to))
    for i in range(3):
        wts[i, t, ds(fx, hid)] = weights[i][ds(z, hid)]
    acc[...] = jnp.zeros_like(acc)
    pre[...] = jnp.zeros_like(pre)

    def sides(g):
        return ((z - g, z >= g, 1), (z + g, z + g < n_z, -1))

    def w_in(i, s):
        w_wait(i, s, z)
        x_copy(i, s).start()
        d_copy(i, 0, s).start()

    last = jnp.where(z < n_z // 2, n_z - 1, 0)

    def x_in(i, s):
        dst = block(i, 1 - fx, s, c)
        rc(dst, dst, x_ss.at[i, s], x_rs.at[i, s], partner).wait_recv()
        d_copy(i, 1, s).start()

    def unit(p, s):
        rows = ds(p, half)
        for i in range(3):
            total = pre[i, rows]
            for k in range(2):
                at = ds(s * 2 + k, cols)
                total += contract_hidden(tok[1 if i == 2 else 0, rows, at], wts[i, s * 2 + k])
            pre[i, rows] = total

    def arrived(i, s):
        for other in range(2):
            side = 1 - fx if other else fx
            dst = block(i, side, s, 1 - c)
            rc(dst, dst, d_ss.at[i, other, s], d_rs.at[i, other, s], partner).wait_recv()

    def finish(g):
        for k, (s, ok, _) in enumerate(sides(g)):
            @pl.when(ok & (s != last))
            def _(k=k, s=s):
                for i in order_i:
                    x_in(i, s)
                for arr in range(2):
                    y_tok_wait(arr, s)
                for i in order_i:
                    arrived(i, s)
                unit(s, s)

                @pl.loop(0, n_z)
                def _(r):
                    dist = jnp.where(r > z, r - z, z - r)
                    known = dist < g
                    if k == 1:
                        known = known | (r == z - g)

                    @pl.when(known)
                    def _():
                        unit(s, r)
                        unit(r, s)

    def w_group(g):
        for i in order_i:
            for s, ok, _ in sides(g):
                @pl.when(ok)
                def _(i=i, s=s):
                    w_in(i, s)

    def w_pass(g):
        for q in range(n_z - g, 0, -1):
            for i in order_i:
                for k, (s, ok, step) in enumerate(sides(g)):
                    e = jnp.where(z // (n_z // 2) == k, q, q - 1)
                    to = z + step * e

                    @pl.when(ok & (e > 0) & (to >= 0) & (to < n_z))
                    def _(i=i, s=s, to=to):
                        w_wait(i, s, to)
                        w_hop(i, s, to, fwd.at[i, s, to])

    for g in range(1, n_z):
        for arr in range(2):
            for s, ok, _ in sides(g):
                @pl.when(ok)
                def _(arr=arr, s=s):
                    tok_in(arr, s)
        if g == 1:
            for i in order_i:
                x_in(i, z)
                arrived(i, z)
            unit(z, z)
        else:
            finish(g - 1)
        if g == 1:
            w_group(g)
            w_pass(g)
        else:
            w_pass(g)
            w_group(g)

    for arr in range(2):
        y_tok_wait(arr, last)

    @pl.loop(0, n_z)
    def _(r):
        @pl.when(r != last)
        def _():
            unit(last, r)

    def part_pre(i, m):
        rows = ds(m, 2 * half)
        total = pre[i, rows]
        for k in range(2):
            at = ds(last * 2 + k, cols)
            total += contract_hidden(tok[1 if i == 2 else 0, rows, at], wts[i, last * 2 + k])
        pre[i, rows] = total

    def whole(i):
        arrived(i, last)
        pl.loop(0, n_z // 2)(lambda m: part_pre(i, m))

    x_in(2, last)
    x_in(0, last)
    whole(2)
    whole(0)
    x_in(1, last)
    arrived(1, last)

    n_cut = 2
    cut = width // n_cut

    def yi_copy(p, n):
        at = ds(n, cut)
        return rc(
            part.at[p, ds(1 - fy, quarter), at], y_in.at[p, :, at],
            yi_ss.at[p, n], yi_rs.at[p, n], dev_y,
        )

    top = z // (n_z // 2)

    def zi_copy(p, n):
        away = p // (n_z // 2) != top
        step = jnp.where(p > z, z + 1, z - 1)
        to = jnp.where(away & (step // (n_z // 2) != top), p, step)
        slot = jnp.where(to != p, p, jnp.where(away, n_z + 1, jnp.where(p < z, n_z, p)))
        at = ds(n, cut)
        return rc(
            part.at[p, ds(fy, quarter), at], z_in.at[slot, :, at],
            zi_ss.at[p, n], zi_rs.at[slot, n], plane(to),
        )

    def zi_wait(slot, n):
        dst = z_in.at[slot, :, ds(n, cut)]
        rc(dst, dst, zi_ss.at[0, n], zi_rs.at[slot, n], partner).wait_recv()

    def sweep(p):
        @pl.loop(0, half // 32)
        def _(r):
            at = ds(p * (half // 32) + r, 32)
            to = ds(r, 32)
            gate_pre, up_pre, hidden_grad = pre[0, at], pre[1, at], pre[2, at]
            sig = jax.nn.sigmoid(gate_pre)
            silu = gate_pre * sig
            hidden_b[to] = (silu * up_pre).astype(BF16)
            gate_g[to] = (hidden_grad * up_pre * sig * (1.0 + gate_pre * (1.0 - sig))).astype(BF16)
            up_g[to] = (hidden_grad * silu).astype(BF16)

        @pl.loop(0, n_cut)
        def _(n):
            for k in range(n_tp // n_cut):
                m = n * (n_tp // n_cut) + k
                part[p, :, ds(m, cols)] = (
                    jnp.dot(gate_g[...], wts[0, m], preferred_element_type=F32)
                    + jnp.dot(up_g[...], wts[1, m], preferred_element_type=F32)
                ).astype(BF16)
            yi_copy(p, n).start()

        @pl.loop(0, 2)
        def _(n):
            at = ds(n, width // 2)
            acc[:, at] += contract_tokens(hidden_b[...], tok[1, ds(p, half), at])

    mine = ds(fy, quarter)

    def yi_wait(p, n):
        dst = y_in.at[p, :, ds(n, cut)]
        rc(dst, dst, yi_ss.at[p, n], yi_rs.at[p, n], dev_y).wait_recv()

    def y_add(p):
        up = jnp.where(p > z, z - 1, z + 1)
        more = (up >= 0) & (up < n_z) & (up // (n_z // 2) == top)

        @pl.loop(0, n_cut)
        def _(n):
            at = ds(n, cut)
            yi_wait(p, n)
            total = part[p, mine, at].astype(F32) + y_in[p, :, at].astype(F32)
            part[p, mine, at] = total.astype(BF16)

            @pl.when(more)
            def _():
                zi_wait(p, n)
                part[p, mine, at] = (total + z_in[p, :, at].astype(F32)).astype(BF16)

            zi_copy(p, n).start()

    def far(k):
        return jnp.where(k == n_z - 1, z, near(n_z - 1 - k))

    outer = (z == 0) | (z == n_z - 1)

    first = far(0) // 2
    part_pre(1, first)

    @pl.loop(0, n_z)
    def _(j):
        sweep(far(j))

        @pl.when(j == 0)
        def _():
            @pl.loop(1, n_z // 2)
            def _(m):
                part_pre(1, (first + m) % (n_z // 2))

        @pl.when((j == n_z - 2) & outer)
        def _():
            y_add(far(0))

    def dn_copy(p):
        return rc(dn_out.at[p], dn_in.at[p], dn_ss.at[p], dn_rs.at[p], partner)

    def dx_copy(p):
        return rc(dx_out.at[p], dx_in.at[p], dx_ss.at[p], dx_rs.at[p], dev_x)

    def dz_copy(p):
        return rc(dz_out.at[p], dz_in.at[z], dz_ss.at[p], dz_rs.at[z], plane(p))

    @pl.loop(0, n_z)
    def _(k):
        p = far(k)
        dn_out[p] = acc[:, ds(p * 2 + 1 - c, cols)].astype(BF16)
        dn_copy(p).start()

    @pl.loop(0, n_z)
    def _(k):
        p = far(k)
        dn_copy(p).wait_recv()
        mine = ds(p * 2 + c, cols)
        other = ds(1 - fx, hid)
        here = ds(fx, hid)
        dx_out[p] = (acc[other, mine] + dn_in[p, other].astype(F32)).astype(BF16)
        dx_copy(p).start()
        acc[here, mine] = acc[here, mine] + dn_in[p, here].astype(F32)

    def down_out(p):
        rows = ds(p, hid)
        return pltpu.make_async_copy(down_ref.at[rows], down_hbm.at[rows], out_sem.at[p])

    def grad_out(i, rows):
        return pltpu.make_async_copy(grad_ref.at[rows], grad_hbm.at[0, rows], out_sem.at[n_z + i])

    def dx_add(p):
        dx_copy(p).wait_recv()
        total = acc[ds(fx, hid), ds(p * 2 + c, cols)] + dx_in[p].astype(F32)

        @pl.when(p == z)
        def _():
            down_ref[ds(z, hid)] = total
            down_out(z).start()

        @pl.when(p != z)
        def _():
            dz_out[p] = total.astype(BF16)
            dz_copy(p).start()

    y_add(far(1))

    @pl.when(jnp.logical_not(outer))
    def _():
        y_add(far(0))

    for k in range(2, n_z - 1):
        y_add(far(k))
    for k in range(n_z - 2):
        dx_add(far(k))

    own_rows = ds(fx * 2 + fy, quarter)
    x_rows = ds((1 - fx) * 2 + fy, quarter)
    y_rows = ds(fx * 2 + 1 - fy, quarter)
    d_rows = ds((1 - fx) * 2 + 1 - fy, quarter)

    def ag_copy(i, n, rows, dev):
        src = grad_ref.at[rows, ds(n, cut)]
        return rc(src, src, ag_ss.at[i, n], ag_rs.at[i, n], dev)

    below = (z > 0) & ((z - 1) // (n_z // 2) == top)
    above = (z < n_z - 1) & ((z + 1) // (n_z // 2) == top)

    @pl.loop(0, n_cut)
    def _(n):
        at = ds(n, cut)

        def gain(slot):
            zi_wait(slot, n)
            total[...] += z_in[slot, :, at].astype(F32)

        yi_wait(z, n)
        total[...] = part[z, mine, at].astype(F32) + y_in[z, :, at].astype(F32)
        gain(n_z + 1)
        pl.when(below)(lambda: gain(z))
        pl.when(above)(lambda: gain(n_z))
        grad_ref[own_rows, at] = total[...].astype(BF16)
        ag_copy(1, n, own_rows, dev_y).start()
        ag_copy(0, n, own_rows, dev_x).start()

    dx_add(far(n_z - 2))

    @pl.loop(0, n_cut)
    def _(n):
        ag_copy(1, n, y_rows, dev_y).wait_recv()
        ag_copy(2, n, y_rows, dev_x).start()

    dx_add(z)

    for j in range(1, n_z):
        s = near(j)
        dst = dz_in.at[s]
        rc(dst, dst, dz_ss.at[s], dz_rs.at[s], partner).wait_recv()
        down_ref[ds(s, hid)] = dz_in[s].astype(F32)
        down_out(s).start()

    grad_out(0, own_rows).start()
    grad_out(1, y_rows).start()
    for n in range(n_cut):
        ag_copy(0, n, x_rows, dev_x).wait_recv()
    grad_out(2, x_rows).start()
    for n in range(n_cut):
        ag_copy(2, n, d_rows, dev_x).wait_recv()
    grad_out(3, d_rows).start()

    for arr in range(2):
        for p in range(n_z):
            @pl.when((z < n_z - 1) & (p <= z))
            def _(arr=arr, p=p):
                z_copy(arr, p, 1).wait_send()

            @pl.when((z > 0) & (p >= z))
            def _(arr=arr, p=p):
                z_copy(arr, p, 0).wait_send()

            @pl.when(p != z)
            def _(arr=arr, p=p):
                y_copy(arr, p).wait_send()

    for p in range(n_z):
        for i in range(3):
            x_copy(i, p).wait_send()
            d_copy(i, 0, p).wait_send()
            d_copy(i, 1, p).wait_send()
        for n in range(n_cut):
            yi_copy(p, n).wait_send()
        dn_copy(p).wait_send()
        dx_copy(p).wait_send()

        @pl.when(p != z)
        def _(p=p):
            for n in range(n_cut):
                zi_copy(p, n).wait_send()
            dz_copy(p).wait_send()

    for s in range(n_z):
        for to in range(n_z):
            if s == to:
                continue

            @pl.when((z >= s) & (z < to) if s < to else (z <= s) & (z > to))
            def _(s=s, to=to):
                for i in range(3):
                    src = fwd.at[i, s, to]
                    rc(src, src, w_ss.at[i, s, to], w_rs.at[i, s, to], partner).wait_send()

    for n in range(n_cut):
        ag_copy(0, n, own_rows, dev_x).wait_send()
        ag_copy(1, n, own_rows, dev_y).wait_send()
        ag_copy(2, n, y_rows, dev_x).wait_send()
    for p in range(n_z):
        down_out(p).wait()
    for i, rows in enumerate((own_rows, y_rows, x_rows, d_rows)):
        grad_out(i, rows).wait()


def spread(n_tp, inputs, cotangent, gate_weight, up_weight, down_weight):
    _, n_tok, width = inputs.shape
    hid_all = gate_weight.shape[1]
    n_z = n_tp // 2
    hid, cols, half, quarter = hid_all // n_z, width // n_tp, n_tok // 2, n_tok // 4
    dma = pltpu.SemaphoreType.DMA
    anyspace = pl.BlockSpec(memory_space=pl.ANY)
    return pl.pallas_call(
        functools.partial(kernel, n_tp),
        name="spread_hidden",
        out_shape=(
            jax.ShapeDtypeStruct((1, n_tok, width), BF16),
            jax.ShapeDtypeStruct((hid_all, cols), F32),
        ),
        in_specs=[anyspace] * 5,
        out_specs=(anyspace, anyspace),
        scratch_shapes=[
            pltpu.VMEM(gate_weight.shape, BF16),
            pltpu.VMEM(up_weight.shape, BF16),
            pltpu.VMEM(down_weight.shape, BF16),
            pltpu.VMEM((n_tok, width), BF16),
            pltpu.VMEM((hid_all, cols), F32),
            pltpu.VMEM((2, n_z * half, width), BF16),
            pltpu.VMEM((3, n_tp, 2 * hid, cols), BF16),
            pltpu.VMEM((hid_all, cols), BF16),
            pltpu.VMEM((hid_all, cols), BF16),
            pltpu.VMEM((n_z, half, width), BF16),
            pltpu.VMEM((n_z, quarter, width), BF16),
            pltpu.VMEM((n_z + 2, quarter, width), BF16),
            pltpu.VMEM((2 * hid, width), F32),
            pltpu.VMEM((3, n_z * half, 2 * hid), F32),
            pltpu.VMEM((half, 2 * hid), BF16),
            pltpu.VMEM((half, 2 * hid), BF16),
            pltpu.VMEM((half, 2 * hid), BF16),
            pltpu.VMEM((quarter, width // 2), F32),
            pltpu.VMEM((n_z, 2 * hid, cols), BF16),
            pltpu.VMEM((n_z, 2 * hid, cols), BF16),
            pltpu.VMEM((n_z, hid, cols), BF16),
            pltpu.VMEM((n_z, hid, cols), BF16),
            pltpu.VMEM((n_z, hid, cols), BF16),
            pltpu.VMEM((n_z, hid, cols), BF16),
            pltpu.VMEM((3, n_z, n_z, hid, cols), BF16),
            dma((5,)), dma((n_z + 4,)), dma((2, n_z, 2)), dma((2, n_z)), dma((2, n_z)), dma((2, n_z)),
            dma((3, n_z, n_z)), dma((3, n_z, n_z)), dma((3, n_z)), dma((3, n_z)),
            dma((3, 2, n_z)), dma((3, 2, n_z)),
            dma((n_z, 2)), dma((n_z, 2)), dma((n_z, 2)), dma((n_z + 2, 2)), dma((3, 2)), dma((3, 2)),
            dma((n_z,)), dma((n_z,)), dma((n_z,)), dma((n_z,)), dma((n_z,)), dma((n_z,)),
        ],
        compiler_params=pltpu.CompilerParams(
            collective_id=0, has_side_effects=True, vmem_limit_bytes=66_000_000
        ),
    )(inputs, cotangent, gate_weight, up_weight, down_weight)


def solution(mesh):
    n_fs, n_tp = mesh.shape["fs"], mesh.shape["tp"]

    def per_device(inputs, cotangent, gate_weight, up_weight, down_weight):
        _, n_tok, width = inputs.shape
        hid_all = gate_weight.shape[1]
        n_z = n_tp // 2
        fits = (
            n_fs == 4
            and n_tp == 2 * n_z
            and hid_all % (n_z * 32) == 0
            and width % (n_tp * 128) == 0
            and n_tok % 64 == 0
            and (3 * n_tok + 9 * hid_all) * n_z * width + 18 * hid_all * width < 62_000_000 * n_z
        )
        if not fits:
            return gathered(inputs, cotangent, gate_weight, up_weight, down_weight)
        return spread(n_tp, inputs, cotangent, gate_weight, up_weight, down_weight)

    return jax.shard_map(
        per_device,
        mesh=mesh,
        in_specs=(
            P("tp", None, None),
            P("tp", None, None),
            P("tp", "fs"),
            P("tp", "fs"),
            P("fs", "tp"),
        ),
        out_specs=(P("tp", None, None), P("fs", "tp")),
        check_vma=False,
    )
```
